256 devices in a mesh: dp: 4 (over x), kv: 32 (over z, y), tp: 2 (over core).
Axes of the slice: x: 4, y: 4, z: 8, core: 2. Of those that a mesh axis runs over, the one named last changes fastest.
Arguments:
- tokens: bfloat16 [16, 2048], P('dp', 'kv'), may hold values from -700 to 700
- norm_gain: float32 [2048], P('kv'), may hold values from 0.1 to 1.9
- w_query: bfloat16 [2048, 2048], P('kv', 'tp'), may hold values from -0.25 to 0.25
- w_key: bfloat16 [2048, 2048], P('kv', 'tp'), may hold values from -0.125 to 0.125
- w_value: bfloat16 [2048, 2048], P('kv', 'tp'), may hold values from -0.125 to 0.125
- w_output: bfloat16 [2048, 2048], P('tp', 'kv'), may hold values from -0.125 to 0.125
- key_cache: bfloat16 [16, 16384, 16, 128], P('dp', 'kv', 'tp'), may hold values from -170 to 170
- value_cache: bfloat16 [16, 16384, 16, 128], P('dp', 'kv', 'tp'), may hold values from -6 to 6
- lengths: int32 [16], P('dp'), may hold values from 8192 to 16383, as said below
- lam: float32 [16], P('tp'), may hold values from 0.3 to 0.8
- head_gain: float32 [128], replicated, may hold values from 0.1 to 1.9
Outputs:
- attended: bfloat16 [16, 2048], P('dp', 'kv')
- new_key: bfloat16 [16, 2048], P('dp', 'tp')
- new_value: bfloat16 [16, 2048], P('dp', 'tp')
The draws below stay inside these ranges and needn't reach their ends.
Inputs may be any that keep to these rules, and one draw needn't show every extreme that they name: `lengths`: exactly one sequence, chosen by the draw, has 16383 past tokens.
All inputs are finite; a program needn't handle non-finite values.
Results may differ from the reference program's by a relative error of at most 0.012.
Values may be sent and summed in bfloat16 or wider, within the bound.
No kernel may reach another device: no remote copies, remote signals or barrier semaphores. Data moves between devices by JAX's collectives and lax.ppermute only.
A program may use at most 64 MiB of HBM per device.

```python
import jax
import jax.numpy as jnp
from jax import lax

D = 2048
HEAD_COUNT = 16
HEAD_WIDTH = 64
POS_DEV = 512
VDIM = 128
BATCH = 16
CACHE_LENGTH = 16384
N_KV = 32
N_TP = 2


def draw_tokens(key, part):
    first = jax.random.fold_in(key, 11)
    second = jax.random.fold_in(key, 12)
    third = jax.random.fold_in(key, 13)
    column = jnp.arange(D, dtype=jnp.float32) / D
    base = jnp.clip(jax.random.normal(first, (BATCH, D), jnp.float32), -4.0, 4.0)
    scales = jnp.exp(2.3 * column + jax.random.uniform(second, (D,), jnp.float32, -0.5, 0.5))
    rows = jnp.exp(jax.random.uniform(third, (BATCH, 1), jnp.float32, 0.0, 2.3))
    return (base * scales[None, :] * rows).astype(jnp.bfloat16)


def draw_key_cache(key, part):
    first = jax.random.fold_in(key, 21)
    base = jnp.clip(jax.random.normal(first, (BATCH, CACHE_LENGTH, HEAD_COUNT, 2 * HEAD_WIDTH), jnp.float32), -4.0, 4.0)
    return base.astype(jnp.bfloat16)


def draw_lengths(key, part):
    first = jax.random.fold_in(key, 31)
    second = jax.random.fold_in(key, 32)
    short = jax.random.randint(first, (BATCH,), 1, CACHE_LENGTH // 2)
    values = CACHE_LENGTH - 1 - short
    chosen = jax.random.randint(second, (), 0, BATCH)
    leading = jnp.arange(BATCH, dtype=jnp.int32) == chosen
    return jnp.where(leading, CACHE_LENGTH - 1, values).astype(jnp.int32)


def steps_of(key, dims, cuts, smallest, top_value):
    gain, own = 1.0, jax.random.fold_in(key, 6)
    for dim, blocks in cuts:
        heights = jnp.exp(jax.random.uniform(jax.random.fold_in(own, dim), (blocks,), jnp.float32, smallest / len(cuts), top_value / len(cuts)))
        gain = gain * jnp.repeat(heights, dims[dim] // blocks).reshape([-1 if axis == dim else 1 for axis in range(len(dims))])
    return gain


def scatter_about(key, dims, scale, most, shards=(), held_as=jnp.bfloat16):
    entries = scale * jax.random.normal(key, dims, jnp.float32)
    if shards:
        entries = entries * steps_of(key, dims, shards, -0.22, 0.18)
    return jnp.clip(entries, -most, most).astype(held_as)


def setup_inputs(seed: int = 0) -> dict:
    key_of = jax.random.split(jax.random.key(seed), 12)
    return {
        "tokens": draw_tokens(jax.random.fold_in(key_of[11], 71), 0),
        "norm_gain": jnp.clip(1.0 + 0.18 * jax.random.normal(key_of[1], (D,), jnp.float32), 0.1, 1.9),
        "w_query": scatter_about(key_of[2], (D, HEAD_COUNT * 2 * HEAD_WIDTH), (1.75 / D ** 0.5), 0.25, ((0, 32), (1, 2))),
        "w_key": scatter_about(key_of[3], (D, HEAD_COUNT * 2 * HEAD_WIDTH), D ** -0.5, 0.125, ((0, 32), (1, 2))),
        "w_value": scatter_about(key_of[4], (D, HEAD_COUNT * VDIM), D ** -0.5, 0.125, ((0, 32), (1, 2))),
        "w_output": scatter_about(key_of[5], (HEAD_COUNT * VDIM, D), (HEAD_COUNT * VDIM) ** -0.5, 0.125, ((0, 2), (1, 32))),
        "key_cache": draw_key_cache(jax.random.fold_in(key_of[11], 71), 0),
        "value_cache": scatter_about(key_of[7], (BATCH, CACHE_LENGTH, HEAD_COUNT, VDIM), 1.0, 6.0, ((0, 4), (1, 32), (2, 2))),
        "lengths": draw_lengths(jax.random.fold_in(key_of[11], 71), 0),
        "lam": jnp.clip(0.3 + 0.5 * jax.random.uniform(key_of[9], (HEAD_COUNT,), jnp.float32) ** steps_of(key_of[9], (HEAD_COUNT,), ((0, 2),), -0.2, 0.2), 0.3, 0.8),
        "head_gain": jnp.clip(1.0 + 0.18 * jax.random.normal(key_of[10], (VDIM,), jnp.float32), 0.1, 1.9),
    }


epsilon = 1e-06

def reference(tokens, norm_gain, w_query, w_key, w_value, w_output, key_cache, value_cache, lengths, lam, head_gain):
    xfull = tokens.astype(jnp.float32)
    inv = lax.rsqrt(lax.optimization_barrier(jnp.mean(xfull * xfull, axis=-1, keepdims=True)) + epsilon)
    scaled = (xfull * norm_gain).astype(jnp.bfloat16)
    query = (jnp.dot(scaled, w_query, preferred_element_type=jnp.float32) * inv).astype(jnp.bfloat16)
    new_key = (jnp.dot(scaled, w_key, preferred_element_type=jnp.float32) * inv).astype(jnp.bfloat16)
    new_value = (jnp.dot(scaled, w_value, preferred_element_type=jnp.float32) * inv).astype(jnp.bfloat16)
    positions = jnp.arange(CACHE_LENGTH, dtype=jnp.int32)

    def one_sequence(items):
        key_cache_rows, vcache, query_row, krow, vrow, length = items
        hit = (positions == length)[:, None, None]
        key_rows = jnp.where(hit, krow.reshape(1, HEAD_COUNT, 2 * HEAD_WIDTH), key_cache_rows)
        values = jnp.where(hit, vrow.reshape(1, HEAD_COUNT, VDIM), vcache)
        logit_score = jnp.einsum('vcb,kvcb->vck', query_row.reshape(HEAD_COUNT, 2, HEAD_WIDTH).astype(jnp.float32), key_rows.reshape(CACHE_LENGTH, HEAD_COUNT, 2, HEAD_WIDTH).astype(jnp.float32)) * HEAD_WIDTH ** (-0.5)
        logit_score = logit_score.reshape(HEAD_COUNT, 2, N_KV, POS_DEV)
        live = (positions <= length).reshape(N_KV, POS_DEV)
        masked = jnp.where(live, logit_score, jnp.float32(-1e+30))
        block_peak = lax.optimization_barrier(jnp.max(masked, axis=-1))
        weights = jnp.where(live, jnp.exp(masked - block_peak[..., None]), jnp.float32(0.0))
        block_sum = lax.optimization_barrier(jnp.sum(weights, axis=-1))
        rounded = weights.astype(jnp.bfloat16).astype(jnp.float32)
        acc = jnp.einsum('hmnp,nphv->hmnv', rounded, values.reshape(N_KV, POS_DEV, HEAD_COUNT, VDIM).astype(jnp.float32))
        top = lax.optimization_barrier(jnp.max(block_peak, axis=-1))
        factor = jnp.exp(block_peak - top[..., None])
        total = lax.optimization_barrier(jnp.sum(block_sum * factor, axis=-1))
        summed = lax.optimization_barrier(jnp.sum(acc * factor[..., None], axis=2))
        return summed[:, 0] / total[:, 0, None] - lam[:, None] * summed[:, 1] / total[:, 1, None]
    mixed = lax.map(one_sequence, (key_cache, value_cache, query, new_key, new_value, lengths))
    heads = mixed * lax.rsqrt(lax.optimization_barrier(jnp.mean(mixed * mixed, axis=-1, keepdims=True)) + epsilon) * head_gain
    heads = heads.astype(jnp.bfloat16).reshape(BATCH, HEAD_COUNT * VDIM)
    half = HEAD_COUNT * VDIM // N_TP
    result = jnp.zeros((BATCH, D), jnp.float32)
    for member in range(N_TP):
        piece = jnp.dot(heads[:, member * half:(member + 1) * half], w_output[member * half:(member + 1) * half], preferred_element_type=jnp.float32).astype(jnp.bfloat16)
        result = result + piece.astype(jnp.float32)
    return (result.astype(jnp.bfloat16), new_key, new_value)
```

```python
import functools

import jax
import jax.numpy as jnp
from jax import lax
from jax.experimental import pallas as pl
from jax.experimental.pallas import tpu as pltpu
from jax.sharding import PartitionSpec as P

D = 2048
HEAD_WIDTH = 64
EPS = 1e-6
NEG = -1e30

ROW_K, ROW_V, ROW_SQ, ROWS_A = 32, 33, 36, 40
ROW_M, ROW_L, ROW_S, ROW_NK, ROW_NV, ROWS_C = 64, 66, 68, 70, 71, 72


def project(tok_ref, gain_ref, wq_ref, wk_ref, wv_ref, out_ref):
    peers = out_ref.shape[0]
    x = tok_ref[...].astype(jnp.float32)
    seqs = x.shape[0]
    squares = jnp.sum(x * x, axis=-1, keepdims=True)
    scaled = (x * gain_ref[...]).astype(jnp.bfloat16)
    heads = wq_ref.shape[1] // 128

    def rows(w_ref):
        y = jnp.dot(scaled, w_ref[...], preferred_element_type=jnp.float32)
        return jnp.concatenate([y[:, h * 128 : (h + 1) * 128] for h in range(heads)], axis=0)

    q, k, v = rows(wq_ref), rows(wk_ref), rows(wv_ref)
    sq = jnp.broadcast_to(squares, (seqs, 128))
    for j in range(peers):
        out_ref[j, 0:32, :] = q
        out_ref[j, ROW_K : ROW_K + 1, :] = k[j : j + 1, :]
        out_ref[j, ROW_V : ROW_V + 1, :] = v[j : j + 1, :]
        out_ref[j, ROW_SQ : ROW_SQ + seqs, :] = sq


def two_pieces(a):
    hi = a.astype(jnp.bfloat16).astype(jnp.float32)
    return hi, (a - hi).astype(jnp.bfloat16).astype(jnp.float32)


def attend(got_ref, key_ref, val_ref, len_ref, out_ref, q_scr, col_scr):
    peers = got_ref.shape[0]
    seqs = key_ref.shape[0]
    width = key_ref.shape[1]
    span = width // 8
    me = lax.axis_index("kv")
    total = got_ref[0]
    for j in range(1, peers):
        total = total + got_ref[j]
    inv = lax.rsqrt(total[ROW_SQ : ROW_SQ + seqs] / D + EPS)
    inv8 = jnp.concatenate([inv, inv], axis=0)
    inv32 = jnp.concatenate([inv8] * 4, axis=0)
    q = (total[0:32] * inv32).astype(jnp.bfloat16).astype(jnp.float32)
    q_scr[...] = q
    seq_id = lax.broadcasted_iota(jnp.int32, (seqs, 128), 0)
    mine = jnp.sum(jnp.where(seq_id == lax.rem(me, seqs), inv, 0.0), axis=0, keepdims=True)
    nk = (total[ROW_K : ROW_K + 1] * mine).astype(jnp.bfloat16)
    nv = (total[ROW_V : ROW_V + 1] * mine).astype(jnp.bfloat16)
    lane = lax.broadcasted_iota(jnp.int32, (8, 128), 1)
    sub = lax.broadcasted_iota(jnp.int32, (8, 128), 0)
    lane1 = lax.broadcasted_iota(jnp.int32, (1, 128), 1)
    qk = q_scr[pl.ds(me, 1), :] * nk.astype(jnp.float32) * HEAD_WIDTH**-0.5
    s1 = jnp.sum(jnp.where(lane1 < HEAD_WIDTH, qk, 0.0), axis=1, keepdims=True)
    s2 = jnp.sum(jnp.where(lane1 >= HEAD_WIDTH, qk, 0.0), axis=1, keepdims=True)
    spot = lax.rem(me, seqs) * 16 + me // seqs
    snew = jnp.where(lane1 == spot, s1, jnp.where(lane1 == spot + 8, s2, NEG))
    own_head = lax.rem(lane, 8) == sub
    col = lax.broadcasted_iota(jnp.int32, (8, width), 1)
    own_head_wide = lax.rem(col, 8) == lax.broadcasted_iota(jnp.int32, (8, width), 0)
    accs = []
    for b in range(seqs):
        qb = q_scr[pl.ds(b, 8, stride=seqs), :] * HEAD_WIDTH**-0.5
        q1 = jnp.where(lane < HEAD_WIDTH, qb, 0.0)
        q2 = jnp.where(lane >= HEAD_WIDTH, qb, 0.0)
        q16 = jnp.concatenate([q1, q2], axis=0).astype(jnp.bfloat16)
        s = lax.dot_general(
            q16, key_ref[b], (((1,), (1,)), ((), ())), preferred_element_type=jnp.float32
        )
        limit = (len_ref[b] - me * span) * 8
        live = jnp.logical_and(own_head_wide, col < limit)
        weights = []
        for m in range(2):
            part = jnp.where(live, s[m * 8 : (m + 1) * 8], NEG)
            hi, lo = two_pieces(jnp.max(part, axis=1, keepdims=True))
            w = jnp.where(live, jnp.exp(part - (hi + lo)), 0.0)
            lhi, llo = two_pieces(jnp.sum(w, axis=1, keepdims=True))
            weights.append(w)
            r = b * 16 + m * 8
            col_scr[r : r + 8, :] = jnp.where(
                lane == 0, hi, jnp.where(lane == 1, lo, jnp.where(lane == 2, lhi, llo))
            )
        w16 = jnp.concatenate(weights, axis=0).astype(jnp.bfloat16)
        accs.append(jnp.dot(w16, val_ref[b], preferred_element_type=jnp.float32))
    turned = jnp.concatenate([col_scr[...], jnp.zeros_like(col_scr)], axis=0).T
    shi, slo = two_pieces(snew)
    tail = jnp.concatenate(
        [turned[0:4], shi, slo, nk.astype(jnp.float32), nv.astype(jnp.float32)], axis=0
    )
    packed = jnp.concatenate(accs + [tail], axis=0).astype(jnp.bfloat16)
    for j in range(peers):
        out_ref[j] = packed


def merge(got_ref, lam_ref, gain_ref, wo_ref, part_ref, nk_ref, nv_ref, head_scr, v_scr):
    peers = got_ref.shape[0]
    seqs = nk_ref.shape[0]

    def row(r):
        return jnp.concatenate(
            [got_ref[j, ROW_M:ROWS_C, :].astype(jnp.float32)[r - ROW_M : r - ROW_M + 1] for j in range(peers)],
            axis=0,
        )

    top = row(ROW_M) + row(ROW_M + 1)
    part = row(ROW_L) + row(ROW_L + 1)
    snew = row(ROW_S) + row(ROW_S + 1)
    peak = jnp.maximum(
        jnp.max(top, axis=0, keepdims=True), jnp.max(snew, axis=0, keepdims=True)
    )
    factor = jnp.exp(top - peak)
    fresh = jnp.sum(jnp.exp(snew - peak), axis=0, keepdims=True)
    total = jnp.sum(part * factor, axis=0, keepdims=True) + fresh
    scale = jnp.concatenate(
        [factor / total, jnp.broadcast_to(fresh / total, (8, 128)), jnp.zeros((88, 128), jnp.float32)],
        axis=0,
    ).T
    nk = row(ROW_NK)
    nv = row(ROW_NV)
    v_scr[...] = nv
    for h in range(8):
        nk_ref[:, h * 128 : (h + 1) * 128] = nk[h * seqs : (h + 1) * seqs].astype(jnp.bfloat16)
        nv_ref[:, h * 128 : (h + 1) * 128] = nv[h * seqs : (h + 1) * seqs].astype(jnp.bfloat16)
    for b in range(seqs):
        maps = []
        fresh_v = v_scr[pl.ds(b, 8, stride=seqs), :]
        for m in range(2):
            r = b * 16 + m * 8
            acc = scale[r : r + 8, peers : peers + 1] * fresh_v
            for j in range(peers):
                acc = acc + scale[r : r + 8, j : j + 1] * got_ref[j, r : r + 8, :].astype(jnp.float32)
            maps.append(acc)
        mixed = maps[0] - lam_ref[...] * maps[1]
        mean = jnp.mean(mixed * mixed, axis=1, keepdims=True)
        head_scr[b * 8 : b * 8 + 8, :] = mixed * lax.rsqrt(mean + EPS) * gain_ref[...]
    heads = jnp.concatenate(
        [head_scr[pl.ds(h, seqs, stride=8), :] for h in range(8)], axis=1
    ).astype(jnp.bfloat16)
    part_ref[...] = jnp.dot(heads, wo_ref[...], preferred_element_type=jnp.float32).astype(
        jnp.bfloat16
    )


VM = pl.BlockSpec(memory_space=pltpu.VMEM)
SM = pl.BlockSpec(memory_space=pltpu.SMEM)


def exchange(array):
    return lax.all_to_all(array, "kv", split_axis=0, concat_axis=0, tiled=True)


def per_device(
    tokens, norm_gain, w_query, w_key, w_value, w_output, key_cache, value_cache, lengths, lam, head_gain
):
    peers = lax.axis_size("kv")
    seqs, span, heads, width = key_cache.shape
    sent = pl.pallas_call(
        project,
        out_shape=jax.ShapeDtypeStruct((peers, ROWS_A, 128), jnp.float32),
        in_specs=[VM] * 5,
        out_specs=VM,
        name="project",
    )(tokens, norm_gain.reshape(1, -1), w_query, w_key, w_value)
    got = exchange(sent)
    sent = pl.pallas_call(
        attend,
        out_shape=jax.ShapeDtypeStruct((peers, ROWS_C, 128), jnp.bfloat16),
        in_specs=[VM, VM, VM, SM],
        out_specs=VM,
        scratch_shapes=[
            pltpu.VMEM((32, 128), jnp.float32),
            pltpu.VMEM((64, 128), jnp.float32),
        ],
        name="attend",
    )(
        got,
        key_cache.reshape(seqs, span * heads, width),
        value_cache.reshape(seqs, span * heads, width),
        lengths,
    )
    got = exchange(sent)
    part, new_key, new_value = pl.pallas_call(
        merge,
        out_shape=(
            jax.ShapeDtypeStruct((seqs, w_output.shape[1]), jnp.bfloat16),
            jax.ShapeDtypeStruct((seqs, heads * width), jnp.bfloat16),
            jax.ShapeDtypeStruct((seqs, heads * width), jnp.bfloat16),
        ),
        in_specs=[VM] * 4,
        out_specs=(VM, VM, VM),
        scratch_shapes=[
            pltpu.VMEM((32, 128), jnp.float32),
            pltpu.VMEM((32, 128), jnp.float32),
        ],
        name="merge",
    )(
        got,
        jnp.broadcast_to(lam[:, None], (heads, 128)),
        head_gain.reshape(1, -1),
        w_output,
    )
    both = lax.all_gather(part, "tp")
    attended = jnp.sum(both.astype(jnp.float32), axis=0).astype(jnp.bfloat16)
    return (attended, new_key, new_value)


def solution(mesh):
    return jax.shard_map(
        per_device,
        mesh=mesh,
        in_specs=(
            P("dp", "kv"),
            P("kv"),
            P("kv", "tp"),
            P("kv", "tp"),
            P("kv", "tp"),
            P("tp", "kv"),
            P("dp", "kv", "tp", None),
            P("dp", "kv", "tp", None),
            P("dp"),
            P("tp"),
            P(),
        ),
        out_specs=(P("dp", "kv"), P("dp", "tp"), P("dp", "tp")),
        check_vma=False,
    )
```

```python
import functools

import jax
import jax.numpy as jnp
from jax import lax
from jax.experimental import pallas as pl
from jax.experimental.pallas import tpu as pltpu
from jax.sharding import PartitionSpec as P

D = 2048
HEAD_WIDTH = 64
EPS = 1e-6
NEG = -1e30

ROW_K, ROW_V, ROW_SQ, ROWS_A = 32, 33, 36, 40
ROW_M, ROW_L, ROW_S, ROW_NK, ROW_NV, ROWS_C = 64, 66, 68, 70, 71, 72


def project(tok_hbm, gain_hbm, wq_hbm, wk_hbm, wv_hbm, out_ref, tok_ref, gain_ref, wq_ref, wk_ref, wv_ref, sems):
    copies = [
        pltpu.make_async_copy(src, dst, sems.at[i])
        for i, (src, dst) in enumerate(
            [(tok_hbm, tok_ref), (gain_hbm, gain_ref), (wq_hbm, wq_ref), (wk_hbm, wk_ref), (wv_hbm, wv_ref)]
        )
    ]
    for c in copies:
        c.start()
    for c in copies:
        c.wait()
    peers = out_ref.shape[0]
    x = tok_ref[...].astype(jnp.float32)
    seqs = x.shape[0]
    squares = jnp.sum(x * x, axis=-1, keepdims=True)
    scaled = (x * gain_ref[...]).astype(jnp.bfloat16)
    heads = wq_ref.shape[1] // 128

    def rows(w_ref):
        y = jnp.dot(scaled, w_ref[...], preferred_element_type=jnp.float32)
        return jnp.concatenate([y[:, h * 128 : (h + 1) * 128] for h in range(heads)], axis=0)

    q, k, v = rows(wq_ref), rows(wk_ref), rows(wv_ref)
    sq = jnp.broadcast_to(squares, (seqs, 128))
    for j in range(peers):
        out_ref[j, 0:32, :] = q
        out_ref[j, ROW_K : ROW_K + 1, :] = k[j : j + 1, :]
        out_ref[j, ROW_V : ROW_V + 1, :] = v[j : j + 1, :]
        out_ref[j, ROW_SQ : ROW_SQ + seqs, :] = sq


def two_pieces(a):
    hi = a.astype(jnp.bfloat16).astype(jnp.float32)
    return hi, (a - hi).astype(jnp.bfloat16).astype(jnp.float32)


def attend(got_ref, key_ref, val_ref, len_ref, out_ref, q_scr, col_scr):
    peers = got_ref.shape[0]
    seqs = key_ref.shape[0]
    width = key_ref.shape[1]
    span = width // 8
    me = lax.axis_index("kv")
    total = got_ref[0]
    for j in range(1, peers):
        total = total + got_ref[j]
    inv = lax.rsqrt(total[ROW_SQ : ROW_SQ + seqs] / D + EPS)
    inv8 = jnp.concatenate([inv, inv], axis=0)
    inv32 = jnp.concatenate([inv8] * 4, axis=0)
    q = (total[0:32] * inv32).astype(jnp.bfloat16).astype(jnp.float32)
    q_scr[...] = q
    seq_id = lax.broadcasted_iota(jnp.int32, (seqs, 128), 0)
    mine = jnp.sum(jnp.where(seq_id == lax.rem(me, seqs), inv, 0.0), axis=0, keepdims=True)
    nk = (total[ROW_K : ROW_K + 1] * mine).astype(jnp.bfloat16)
    nv = (total[ROW_V : ROW_V + 1] * mine).astype(jnp.bfloat16)
    lane = lax.broadcasted_iota(jnp.int32, (8, 128), 1)
    sub = lax.broadcasted_iota(jnp.int32, (8, 128), 0)
    lane1 = lax.broadcasted_iota(jnp.int32, (1, 128), 1)
    qk = q_scr[pl.ds(me, 1), :] * nk.astype(jnp.float32) * HEAD_WIDTH**-0.5
    s1 = jnp.sum(jnp.where(lane1 < HEAD_WIDTH, qk, 0.0), axis=1, keepdims=True)
    s2 = jnp.sum(jnp.where(lane1 >= HEAD_WIDTH, qk, 0.0), axis=1, keepdims=True)
    spot = lax.rem(me, seqs) * 16 + me // seqs
    snew = jnp.where(lane1 == spot, s1, jnp.where(lane1 == spot + 8, s2, NEG))
    own_head = lax.rem(lane, 8) == sub
    col = lax.broadcasted_iota(jnp.int32, (8, width), 1)
    own_head_wide = lax.rem(col, 8) == lax.broadcasted_iota(jnp.int32, (8, width), 0)
    accs = []
    for b in range(seqs):
        qb = q_scr[pl.ds(b, 8, stride=seqs), :] * HEAD_WIDTH**-0.5
        q1 = jnp.where(lane < HEAD_WIDTH, qb, 0.0)
        q2 = jnp.where(lane >= HEAD_WIDTH, qb, 0.0)
        q16 = jnp.concatenate([q1, q2], axis=0).astype(jnp.bfloat16)
        s = lax.dot_general(
            q16, key_ref[b], (((1,), (1,)), ((), ())), preferred_element_type=jnp.float32
        )
        limit = (len_ref[b] - me * span) * 8
        live = jnp.logical_and(own_head_wide, col < limit)
        weights = []
        for m in range(2):
            part = jnp.where(live, s[m * 8 : (m + 1) * 8], NEG)
            hi, lo = two_pieces(jnp.max(part, axis=1, keepdims=True))
            w = jnp.where(live, jnp.exp(part - (hi + lo)), 0.0)
            lhi, llo = two_pieces(jnp.sum(w, axis=1, keepdims=True))
            weights.append(w)
            r = b * 16 + m * 8
            col_scr[r : r + 8, :] = jnp.where(
                lane == 0, hi, jnp.where(lane == 1, lo, jnp.where(lane == 2, lhi, llo))
            )
        w16 = jnp.concatenate(weights, axis=0).astype(jnp.bfloat16)
        accs.append(jnp.dot(w16, val_ref[b], preferred_element_type=jnp.float32))
    turned = jnp.concatenate([col_scr[...], jnp.zeros_like(col_scr)], axis=0).T
    shi, slo = two_pieces(snew)
    tail = jnp.concatenate(
        [turned[0:4], shi, slo, nk.astype(jnp.float32), nv.astype(jnp.float32)], axis=0
    )
    packed = jnp.concatenate(accs + [tail], axis=0).astype(jnp.bfloat16)
    for j in range(peers):
        out_ref[j] = packed


def merge(got_ref, lam_ref, gain_ref, wo_ref, part_ref, nk_ref, nv_ref, head_scr, v_scr):
    peers = got_ref.shape[0]
    seqs = nk_ref.shape[0]

    def row(r):
        return jnp.concatenate(
            [got_ref[j, ROW_M:ROWS_C, :].astype(jnp.float32)[r - ROW_M : r - ROW_M + 1] for j in range(peers)],
            axis=0,
        )

    top = row(ROW_M) + row(ROW_M + 1)
    part = row(ROW_L) + row(ROW_L + 1)
    snew = row(ROW_S) + row(ROW_S + 1)
    peak = jnp.maximum(
        jnp.max(top, axis=0, keepdims=True), jnp.max(snew, axis=0, keepdims=True)
    )
    factor = jnp.exp(top - peak)
    fresh = jnp.sum(jnp.exp(snew - peak), axis=0, keepdims=True)
    total = jnp.sum(part * factor, axis=0, keepdims=True) + fresh
    scale = jnp.concatenate(
        [factor / total, jnp.broadcast_to(fresh / total, (8, 128)), jnp.zeros((88, 128), jnp.float32)],
        axis=0,
    ).T
    nk = row(ROW_NK)
    nv = row(ROW_NV)
    v_scr[...] = nv
    for h in range(8):
        nk_ref[:, h * 128 : (h + 1) * 128] = nk[h * seqs : (h + 1) * seqs].astype(jnp.bfloat16)
        nv_ref[:, h * 128 : (h + 1) * 128] = nv[h * seqs : (h + 1) * seqs].astype(jnp.bfloat16)
    sub = lax.broadcasted_iota(jnp.int32, (8, 128), 0)
    lam = jnp.zeros((8, 128), jnp.float32)
    for h in range(8):
        lam = jnp.where(sub == h, lam_ref[h], lam)
    for b in range(seqs):
        maps = []
        fresh_v = v_scr[pl.ds(b, 8, stride=seqs), :]
        for m in range(2):
            r = b * 16 + m * 8
            acc = scale[r : r + 8, peers : peers + 1] * fresh_v
            for j in range(peers):
                acc = acc + scale[r : r + 8, j : j + 1] * got_ref[j, r : r + 8, :].astype(jnp.float32)
            maps.append(acc)
        mixed = maps[0] - lam * maps[1]
        mean = jnp.mean(mixed * mixed, axis=1, keepdims=True)
        head_scr[b * 8 : b * 8 + 8, :] = mixed * lax.rsqrt(mean + EPS) * gain_ref[...]
    heads = jnp.concatenate(
        [head_scr[pl.ds(h, seqs, stride=8), :] for h in range(8)], axis=1
    ).astype(jnp.bfloat16)
    part_ref[...] = lax.dot_general(
        heads, wo_ref[...], (((1,), (1,)), ((), ())), preferred_element_type=jnp.float32
    ).astype(jnp.bfloat16)


VM = pl.BlockSpec(memory_space=pltpu.VMEM)
SM = pl.BlockSpec(memory_space=pltpu.SMEM)


def exchange(array):
    return lax.all_to_all(array, "kv", split_axis=0, concat_axis=0, tiled=True)


def per_device(
    tokens, norm_gain, w_query, w_key, w_value, w_output, key_cache, value_cache, lengths, lam, head_gain
):
    peers = lax.axis_size("kv")
    seqs, span, heads, width = key_cache.shape
    sent = pl.pallas_call(
        project,
        out_shape=jax.ShapeDtypeStruct((peers, ROWS_A, 128), jnp.float32),
        in_specs=[pl.BlockSpec(memory_space=pltpu.HBM)] * 5,
        out_specs=VM,
        scratch_shapes=[
            pltpu.VMEM(tokens.shape, jnp.bfloat16),
            pltpu.VMEM((1, norm_gain.shape[0]), jnp.float32),
            pltpu.VMEM(w_query.shape, jnp.bfloat16),
            pltpu.VMEM(w_query.shape, jnp.bfloat16),
            pltpu.VMEM(w_query.shape, jnp.bfloat16),
            pltpu.SemaphoreType.DMA((5,)),
        ],
        name="project",
        cost_estimate=pl.CostEstimate(flops=5_000_000_000, bytes_accessed=30_000_000, transcendentals=0),
        compiler_params=pltpu.CompilerParams(vmem_limit_bytes=8 << 20),
    )(*(pltpu.with_memory_space_constraint(a, pltpu.HBM) for a in (tokens, norm_gain.reshape(1, -1), w_query, w_key, w_value)))
    got = exchange(sent)
    sent = pl.pallas_call(
        attend,
        out_shape=jax.ShapeDtypeStruct((peers, ROWS_C, 128), jnp.bfloat16),
        in_specs=[VM, VM, VM, SM],
        out_specs=VM,
        scratch_shapes=[
            pltpu.VMEM((32, 128), jnp.float32),
            pltpu.VMEM((64, 128), jnp.float32),
        ],
        name="attend",
        compiler_params=pltpu.CompilerParams(vmem_limit_bytes=24 << 20),
    )(
        got,
        key_cache.reshape(seqs, span * heads, width),
        value_cache.reshape(seqs, span * heads, width),
        lengths,
    )
    got = exchange(sent)
    part, new_key, new_value = pl.pallas_call(
        merge,
        out_shape=(
            jax.ShapeDtypeStruct((seqs, w_output.shape[1]), jnp.bfloat16),
            jax.ShapeDtypeStruct((seqs, heads * width), jnp.bfloat16),
            jax.ShapeDtypeStruct((seqs, heads * width), jnp.bfloat16),
        ),
        in_specs=[VM, SM, VM, VM],
        out_specs=(VM, VM, VM),
        scratch_shapes=[
            pltpu.VMEM((32, 128), jnp.float32),
            pltpu.VMEM((32, 128), jnp.float32),
        ],
        name="merge",
        compiler_params=pltpu.CompilerParams(vmem_limit_bytes=8 << 20),
    )(
        got,
        lam,
        head_gain.reshape(1, -1),
        w_output.T,
    )
    both = lax.all_gather(part, "tp")
    attended = jnp.sum(both.astype(jnp.float32), axis=0).astype(jnp.bfloat16)
    return (attended, new_key, new_value)


def solution(mesh):
    return jax.shard_map(
        per_device,
        mesh=mesh,
        in_specs=(
            P("dp", "kv"),
            P("kv"),
            P("kv", "tp"),
            P("kv", "tp"),
            P("kv", "tp"),
            P("tp", "kv"),
            P("dp", "kv", "tp", None),
            P("dp", "kv", "tp", None),
            P("dp"),
            P("tp"),
            P(),
        ),
        out_specs=(P("dp", "kv"), P("dp", "tp"), P("dp", "tp")),
        check_vma=False,
    )
```

```python
import functools

import jax
import jax.numpy as jnp
from jax import lax
from jax.experimental import pallas as pl
from jax.experimental.pallas import tpu as pltpu
from jax.sharding import PartitionSpec as P

D = 2048
HEAD_WIDTH = 64
EPS = 1e-6
NEG = -1e30

ROWS_A, BITS = 40, 14.5
ROW_M, ROW_L, ROW_S, ROW_NK, ROW_NV, ROWS_C = 64, 66, 68, 70, 71, 72


def exponent(a):
    return jnp.ceil(jnp.log2(jnp.maximum(a, 1e-30)))


def project(tok_hbm, gain_hbm, wq_hbm, wk_hbm, wv_hbm, out_ref, tok_ref, gain_ref, wq_ref, wk_ref, wv_ref, sems):
    copies = [
        pltpu.make_async_copy(src, dst, sems.at[i])
        for i, (src, dst) in enumerate(
            [(tok_hbm, tok_ref), (gain_hbm, gain_ref), (wq_hbm, wq_ref), (wk_hbm, wk_ref), (wv_hbm, wv_ref)]
        )
    ]
    for c in copies:
        c.start()
    for c in copies:
        c.wait()
    peers = out_ref.shape[0]
    x = tok_ref[...].astype(jnp.float32)
    seqs = x.shape[0]
    squares = jnp.sum(x * x, axis=-1, keepdims=True)
    scaled = (x * gain_ref[...]).astype(jnp.bfloat16)
    heads = wq_ref.shape[1] // 128

    def rows(w_ref):
        y = jnp.dot(scaled, w_ref[...], preferred_element_type=jnp.float32)
        e = exponent(jnp.max(jnp.abs(y), axis=1, keepdims=True))
        y = jnp.round(y * jnp.exp2(BITS - e))
        return jnp.concatenate([y[:, h * 128 : (h + 1) * 128] for h in range(heads)], axis=0), e

    (q, qe), (k, ke), (v, ve) = rows(wq_ref), rows(wk_ref), rows(wv_ref)
    se = exponent(squares)
    size = squares * jnp.exp2(BITS - se)
    whole = jnp.floor(size)
    rest = jnp.round((size - whole) * 2.0**14)
    lane = lax.broadcasted_iota(jnp.int32, (seqs, 128), 1)
    meta = jnp.where(
        lane == 0, qe, jnp.where(lane == 1, se, jnp.where(lane == 2, whole, rest))
    )
    q = q.astype(jnp.int32).astype(jnp.int16)
    for j in range(peers):
        b = j % seqs
        tile = jnp.concatenate(
            [
                k[j : j + 1],
                v[j : j + 1],
                jnp.broadcast_to(ke[b : b + 1], (1, 128)),
                jnp.broadcast_to(ve[b : b + 1], (1, 128)),
                meta,
            ],
            axis=0,
        )
        out_ref[j, 0:32, :] = q
        out_ref[j, 32:40, :] = tile.astype(jnp.int32).astype(jnp.int16)


def two_pieces(a):
    hi = a.astype(jnp.bfloat16).astype(jnp.float32)
    return hi, (a - hi).astype(jnp.bfloat16).astype(jnp.float32)


def attend(got_ref, key_ref, val_ref, len_ref, out_ref, q_scr, col_scr):
    peers = got_ref.shape[0]
    seqs = key_ref.shape[0]
    width = key_ref.shape[1]
    span = width // 8
    me = lax.axis_index("kv")
    total = [jnp.zeros((8, 128), jnp.float32)] * 4
    own = jnp.zeros((8, 128), jnp.float32)
    squares = jnp.zeros((8, 128), jnp.float32)
    for j in range(peers):
        got = got_ref[j].astype(jnp.int32).astype(jnp.float32)
        tile = got[32:40]
        unit = jnp.exp2(tile - BITS)
        units = jnp.concatenate([unit[4:8, 0:1]] * 2, axis=0)
        total = [t + got[i * 8 : i * 8 + 8] * units for i, t in enumerate(total)]
        own = own + tile * pltpu.roll(unit, 6, 0)
        size = tile + pltpu.roll(tile, 127, 1) * 2.0**-14
        squares = squares + size * pltpu.roll(unit, 1, 1)
    total = jnp.concatenate(total, axis=0)
    inv = lax.rsqrt(jnp.broadcast_to(squares[4:8, 2:3], (4, 128)) / D + EPS)
    inv8 = jnp.concatenate([inv, inv], axis=0)
    inv32 = jnp.concatenate([inv8] * 4, axis=0)
    q = (total * inv32).astype(jnp.bfloat16).astype(jnp.float32)
    q_scr[...] = q
    seq_id = lax.broadcasted_iota(jnp.int32, (seqs, 128), 0)
    mine = jnp.sum(jnp.where(seq_id == lax.rem(me, seqs), inv, 0.0), axis=0, keepdims=True)
    nk = (own[0:1] * mine).astype(jnp.bfloat16)
    nv = (own[1:2] * mine).astype(jnp.bfloat16)
    lane = lax.broadcasted_iota(jnp.int32, (8, 128), 1)
    sub = lax.broadcasted_iota(jnp.int32, (8, 128), 0)
    lane1 = lax.broadcasted_iota(jnp.int32, (1, 128), 1)
    qk = q_scr[pl.ds(me, 1), :] * nk.astype(jnp.float32) * HEAD_WIDTH**-0.5
    s1 = jnp.sum(jnp.where(lane1 < HEAD_WIDTH, qk, 0.0), axis=1, keepdims=True)
    s2 = jnp.sum(jnp.where(lane1 >= HEAD_WIDTH, qk, 0.0), axis=1, keepdims=True)
    spot = lax.rem(me, seqs) * 16 + me // seqs
    snew = jnp.where(lane1 == spot, s1, jnp.where(lane1 == spot + 8, s2, NEG))
    own_head = lax.rem(lane, 8) == sub
    col = lax.broadcasted_iota(jnp.int32, (8, width), 1)
    own_head_wide = lax.rem(col, 8) == lax.broadcasted_iota(jnp.int32, (8, width), 0)
    accs = []
    for b in range(seqs):
        qb = q_scr[pl.ds(b, 8, stride=seqs), :] * HEAD_WIDTH**-0.5
        q1 = jnp.where(lane < HEAD_WIDTH, qb, 0.0)
        q2 = jnp.where(lane >= HEAD_WIDTH, qb, 0.0)
        q16 = jnp.concatenate([q1, q2], axis=0).astype(jnp.bfloat16)
        s = lax.dot_general(
            q16, key_ref[b], (((1,), (1,)), ((), ())), preferred_element_type=jnp.float32
        )
        limit = (len_ref[b] - me * span) * 8
        live = jnp.logical_and(own_head_wide, col < limit)
        weights = []
        for m in range(2):
            part = jnp.where(live, s[m * 8 : (m + 1) * 8], NEG)
            hi, lo = two_pieces(jnp.max(part, axis=1, keepdims=True))
            w = jnp.where(live, jnp.exp(part - (hi + lo)), 0.0)
            lhi, llo = two_pieces(jnp.sum(w, axis=1, keepdims=True))
            weights.append(w)
            r = b * 16 + m * 8
            col_scr[r : r + 8, :] = jnp.where(
                lane == 0, hi, jnp.where(lane == 1, lo, jnp.where(lane == 2, lhi, llo))
            )
        w16 = jnp.concatenate(weights, axis=0).astype(jnp.bfloat16)
        accs.append(jnp.dot(w16, val_ref[b], preferred_element_type=jnp.float32))
    turned = jnp.concatenate([col_scr[...], jnp.zeros_like(col_scr)], axis=0).T
    shi, slo = two_pieces(snew)
    tail = jnp.concatenate(
        [turned[0:4], shi, slo, nk.astype(jnp.float32), nv.astype(jnp.float32)], axis=0
    )
    packed = jnp.concatenate(accs + [tail], axis=0).astype(jnp.bfloat16)
    for j in range(peers):
        out_ref[j] = packed


def merge(got_ref, lam_ref, gain_ref, wo_ref, part_ref, nk_ref, nv_ref, head_scr, v_scr):
    peers = got_ref.shape[0]
    seqs = nk_ref.shape[0]

    def row(r):
        return jnp.concatenate(
            [got_ref[j, ROW_M:ROWS_C, :].astype(jnp.float32)[r - ROW_M : r - ROW_M + 1] for j in range(peers)],
            axis=0,
        )

    top = row(ROW_M) + row(ROW_M + 1)
    part = row(ROW_L) + row(ROW_L + 1)
    snew = row(ROW_S) + row(ROW_S + 1)
    peak = jnp.maximum(
        jnp.max(top, axis=0, keepdims=True), jnp.max(snew, axis=0, keepdims=True)
    )
    factor = jnp.exp(top - peak)
    fresh = jnp.sum(jnp.exp(snew - peak), axis=0, keepdims=True)
    total = jnp.sum(part * factor, axis=0, keepdims=True) + fresh
    scale = jnp.concatenate(
        [factor / total, jnp.broadcast_to(fresh / total, (8, 128)), jnp.zeros((88, 128), jnp.float32)],
        axis=0,
    ).T
    nk = row(ROW_NK)
    nv = row(ROW_NV)
    v_scr[...] = nv
    for h in range(8):
        nk_ref[:, h * 128 : (h + 1) * 128] = nk[h * seqs : (h + 1) * seqs].astype(jnp.bfloat16)
        nv_ref[:, h * 128 : (h + 1) * 128] = nv[h * seqs : (h + 1) * seqs].astype(jnp.bfloat16)
    sub = lax.broadcasted_iota(jnp.int32, (8, 128), 0)
    lam = jnp.zeros((8, 128), jnp.float32)
    for h in range(8):
        lam = jnp.where(sub == h, lam_ref[h], lam)
    for b in range(seqs):
        maps = []
        fresh_v = v_scr[pl.ds(b, 8, stride=seqs), :]
        for m in range(2):
            r = b * 16 + m * 8
            acc = scale[r : r + 8, peers : peers + 1] * fresh_v
            for j in range(peers):
                acc = acc + scale[r : r + 8, j : j + 1] * got_ref[j, r : r + 8, :].astype(jnp.float32)
            maps.append(acc)
        mixed = maps[0] - lam * maps[1]
        mean = jnp.mean(mixed * mixed, axis=1, keepdims=True)
        head_scr[b * 8 : b * 8 + 8, :] = mixed * lax.rsqrt(mean + EPS) * gain_ref[...]
    heads = jnp.concatenate(
        [head_scr[pl.ds(h, seqs, stride=8), :] for h in range(8)], axis=1
    ).astype(jnp.bfloat16)
    part_ref[...] = lax.dot_general(
        heads, wo_ref[...], (((1,), (1,)), ((), ())), preferred_element_type=jnp.float32
    ).astype(jnp.bfloat16)


VM = pl.BlockSpec(memory_space=pltpu.VMEM)
SM = pl.BlockSpec(memory_space=pltpu.SMEM)


def exchange(array):
    return lax.all_to_all(array, "kv", split_axis=0, concat_axis=0, tiled=True)


def per_device(
    tokens, norm_gain, w_query, w_key, w_value, w_output, key_cache, value_cache, lengths, lam, head_gain
):
    peers = lax.axis_size("kv")
    seqs, span, heads, width = key_cache.shape
    sent = pl.pallas_call(
        project,
        out_shape=jax.ShapeDtypeStruct((peers, ROWS_A, 128), jnp.int16),
        in_specs=[pl.BlockSpec(memory_space=pltpu.HBM)] * 5,
        out_specs=VM,
        scratch_shapes=[
            pltpu.VMEM(tokens.shape, jnp.bfloat16),
            pltpu.VMEM((1, norm_gain.shape[0]), jnp.float32),
            pltpu.VMEM(w_query.shape, jnp.bfloat16),
            pltpu.VMEM(w_query.shape, jnp.bfloat16),
            pltpu.VMEM(w_query.shape, jnp.bfloat16),
            pltpu.SemaphoreType.DMA((5,)),
        ],
        name="project",
        cost_estimate=pl.CostEstimate(flops=5_000_000_000, bytes_accessed=30_000_000, transcendentals=0),
        compiler_params=pltpu.CompilerParams(vmem_limit_bytes=8 << 20),
    )(*(pltpu.with_memory_space_constraint(a, pltpu.HBM) for a in (tokens, norm_gain.reshape(1, -1), w_query, w_key, w_value)))
    got = exchange(sent)
    sent = pl.pallas_call(
        attend,
        out_shape=jax.ShapeDtypeStruct((peers, ROWS_C, 128), jnp.bfloat16),
        in_specs=[VM, VM, VM, SM],
        out_specs=VM,
        scratch_shapes=[
            pltpu.VMEM((32, 128), jnp.float32),
            pltpu.VMEM((64, 128), jnp.float32),
        ],
        name="attend",
        compiler_params=pltpu.CompilerParams(vmem_limit_bytes=24 << 20),
    )(
        got,
        key_cache.reshape(seqs, span * heads, width),
        value_cache.reshape(seqs, span * heads, width),
        lengths,
    )
    got = exchange(sent)
    part, new_key, new_value = pl.pallas_call(
        merge,
        out_shape=(
            jax.ShapeDtypeStruct((seqs, w_output.shape[1]), jnp.bfloat16),
            jax.ShapeDtypeStruct((seqs, heads * width), jnp.bfloat16),
            jax.ShapeDtypeStruct((seqs, heads * width), jnp.bfloat16),
        ),
        in_specs=[VM, SM, VM, VM],
        out_specs=(VM, VM, VM),
        scratch_shapes=[
            pltpu.VMEM((32, 128), jnp.float32),
            pltpu.VMEM((32, 128), jnp.float32),
        ],
        name="merge",
        compiler_params=pltpu.CompilerParams(vmem_limit_bytes=8 << 20),
    )(
        got,
        lam,
        head_gain.reshape(1, -1),
        w_output.T,
    )
    both = lax.all_gather(part, "tp")
    attended = jnp.sum(both.astype(jnp.float32), axis=0).astype(jnp.bfloat16)
    return (attended, new_key, new_value)


def solution(mesh):
    return jax.shard_map(
        per_device,
        mesh=mesh,
        in_specs=(
            P("dp", "kv"),
            P("kv"),
            P("kv", "tp"),
            P("kv", "tp"),
            P("kv", "tp"),
            P("tp", "kv"),
            P("dp", "kv", "tp", None),
            P("dp", "kv", "tp", None),
            P("dp"),
            P("tp"),
            P(),
        ),
        out_specs=(P("dp", "kv"), P("dp", "tp"), P("dp", "tp")),
        check_vma=False,
    )
```

```python
import jax
import jax.numpy as jnp
from jax import lax
from jax.experimental import pallas as pl
from jax.experimental.pallas import tpu as pltpu
from jax.sharding import Mesh
from jax.sharding import PartitionSpec as P

D = 2048
HEAD_WIDTH = 64
EPS = 1e-6
NEG = -1e30

ROWS_A, BITS = 40, 14.5
ROW_M, ROW_L, ROW_S, ROW_NK, ROW_NV, ROWS_C = 64, 66, 68, 70, 71, 72
ROW_NKS, ROW_NVS, ROWS_E = 72, 80, 88

def exponent(a):
    return jnp.ceil(jnp.log2(jnp.maximum(a, 1e-30)))


def project(tok_hbm, gain_hbm, wq_hbm, wk_hbm, wv_hbm, out_ref, tok_ref, gain_ref, wq_ref, wk_ref, wv_ref, sems):
    copies = [
        pltpu.make_async_copy(src, dst, sems.at[i])
        for i, (src, dst) in enumerate(
            [(tok_hbm, tok_ref), (gain_hbm, gain_ref), (wq_hbm, wq_ref), (wk_hbm, wk_ref), (wv_hbm, wv_ref)]
        )
    ]
    for c in copies:
        c.start()
    for c in copies:
        c.wait()
    peers = out_ref.shape[0]
    x = tok_ref[...].astype(jnp.float32)
    seqs = x.shape[0]
    squares = jnp.sum(x * x, axis=-1, keepdims=True)
    scaled = (x * gain_ref[...]).astype(jnp.bfloat16)
    heads = wq_ref.shape[1] // 128

    def rows(w_ref):
        y = jnp.dot(scaled, w_ref[...], preferred_element_type=jnp.float32)
        e = exponent(jnp.max(jnp.abs(y), axis=1, keepdims=True))
        y = jnp.round(y * jnp.exp2(BITS - e))
        return jnp.concatenate([y[:, h * 128 : (h + 1) * 128] for h in range(heads)], axis=0), e

    (q, qe), (k, ke), (v, ve) = rows(wq_ref), rows(wk_ref), rows(wv_ref)
    se = exponent(squares)
    size = squares * jnp.exp2(BITS - se)
    whole = jnp.floor(size)
    rest = jnp.round((size - whole) * 2.0**14)
    lane = lax.broadcasted_iota(jnp.int32, (seqs, 128), 1)
    meta = jnp.where(
        lane == 0, qe, jnp.where(lane == 1, se, jnp.where(lane == 2, whole, rest))
    )
    q = q.astype(jnp.int32).astype(jnp.int16)
    for j in range(peers):
        b = j % seqs
        tile = jnp.concatenate(
            [
                k[j : j + 1],
                v[j : j + 1],
                jnp.broadcast_to(ke[b : b + 1], (1, 128)),
                jnp.broadcast_to(ve[b : b + 1], (1, 128)),
                meta,
            ],
            axis=0,
        )
        out_ref[j, 0:32, :] = q
        out_ref[j, 32:40, :] = tile.astype(jnp.int32).astype(jnp.int16)


def two_pieces(a):
    hi = a.astype(jnp.bfloat16).astype(jnp.float32)
    return hi, (a - hi).astype(jnp.bfloat16).astype(jnp.float32)


def attend(got_ref, key_ref, val_ref, len_ref, out_ref, q_scr, col_scr):
    peers = got_ref.shape[0]
    seqs = key_ref.shape[0]
    width = key_ref.shape[1]
    span = width // 8
    me = lax.axis_index("kv_0") * lax.axis_size("kv_1") + lax.axis_index("kv_1")
    total = [jnp.zeros((8, 128), jnp.float32)] * 4
    own = jnp.zeros((8, 128), jnp.float32)
    squares = jnp.zeros((8, 128), jnp.float32)
    for j in range(peers):
        got = got_ref[j].astype(jnp.int32).astype(jnp.float32)
        tile = got[32:40]
        unit = jnp.exp2(tile - BITS)
        units = jnp.concatenate([unit[4:8, 0:1]] * 2, axis=0)
        total = [t + got[i * 8 : i * 8 + 8] * units for i, t in enumerate(total)]
        own = own + tile * pltpu.roll(unit, 6, 0)
        size = tile + pltpu.roll(tile, 127, 1) * 2.0**-14
        squares = squares + size * pltpu.roll(unit, 1, 1)
    total = jnp.concatenate(total, axis=0)
    inv = lax.rsqrt(jnp.broadcast_to(squares[4:8, 2:3], (4, 128)) / D + EPS)
    inv8 = jnp.concatenate([inv, inv], axis=0)
    inv32 = jnp.concatenate([inv8] * 4, axis=0)
    q = (total * inv32).astype(jnp.bfloat16).astype(jnp.float32)
    q_scr[...] = q
    seq_id = lax.broadcasted_iota(jnp.int32, (seqs, 128), 0)
    mine = jnp.sum(jnp.where(seq_id == lax.rem(me, seqs), inv, 0.0), axis=0, keepdims=True)
    nk = (own[0:1] * mine).astype(jnp.bfloat16)
    nv = (own[1:2] * mine).astype(jnp.bfloat16)
    lane = lax.broadcasted_iota(jnp.int32, (8, 128), 1)
    sub = lax.broadcasted_iota(jnp.int32, (8, 128), 0)
    lane1 = lax.broadcasted_iota(jnp.int32, (1, 128), 1)
    qk = q_scr[pl.ds(me, 1), :] * nk.astype(jnp.float32) * HEAD_WIDTH**-0.5
    s1 = jnp.sum(jnp.where(lane1 < HEAD_WIDTH, qk, 0.0), axis=1, keepdims=True)
    s2 = jnp.sum(jnp.where(lane1 >= HEAD_WIDTH, qk, 0.0), axis=1, keepdims=True)
    spot = lax.rem(me, seqs) * 16 + me // seqs
    snew = jnp.where(lane1 == spot, s1, jnp.where(lane1 == spot + 8, s2, NEG))
    own_head = lax.rem(lane, 8) == sub
    col = lax.broadcasted_iota(jnp.int32, (8, width), 1)
    own_head_wide = lax.rem(col, 8) == lax.broadcasted_iota(jnp.int32, (8, width), 0)
    accs = []
    for b in range(seqs):
        qb = q_scr[pl.ds(b, 8, stride=seqs), :] * HEAD_WIDTH**-0.5
        q1 = jnp.where(lane < HEAD_WIDTH, qb, 0.0)
        q2 = jnp.where(lane >= HEAD_WIDTH, qb, 0.0)
        q16 = jnp.concatenate([q1, q2], axis=0).astype(jnp.bfloat16)
        s = lax.dot_general(
            q16, key_ref[b], (((1,), (1,)), ((), ())), preferred_element_type=jnp.float32
        )
        limit = (len_ref[b] - me * span) * 8
        live = jnp.logical_and(own_head_wide, col < limit)
        weights = []
        for m in range(2):
            part = jnp.where(live, s[m * 8 : (m + 1) * 8], NEG)
            hi, lo = two_pieces(jnp.max(part, axis=1, keepdims=True))
            w = jnp.where(live, jnp.exp(part - (hi + lo)), 0.0)
            lhi, llo = two_pieces(jnp.sum(w, axis=1, keepdims=True))
            weights.append(w)
            r = b * 16 + m * 8
            col_scr[r : r + 8, :] = jnp.where(
                lane == 0, hi, jnp.where(lane == 1, lo, jnp.where(lane == 2, lhi, llo))
            )
        w16 = jnp.concatenate(weights, axis=0).astype(jnp.bfloat16)
        accs.append(jnp.dot(w16, val_ref[b], preferred_element_type=jnp.float32))
    turned = jnp.concatenate([col_scr[...], jnp.zeros_like(col_scr)], axis=0).T
    shi, slo = two_pieces(snew)
    tail = jnp.concatenate(
        [turned[0:4], shi, slo, nk.astype(jnp.float32), nv.astype(jnp.float32)], axis=0
    )
    packed = jnp.concatenate(accs + [tail], axis=0).astype(jnp.bfloat16)
    for j in range(out_ref.shape[0]):
        out_ref[j] = packed


def tails(got_ref):
    peers = got_ref.shape[0]
    tiles = [got_ref[j, ROW_M : ROW_M + 8, :].astype(jnp.float32) for j in range(peers)]
    return lambda r: jnp.concatenate([t[r - ROW_M : r - ROW_M + 1] for t in tiles], axis=0)


def columns(rows):
    used = sum(r.shape[0] for r in rows)
    return jnp.concatenate(rows + [jnp.zeros((128 - used, 128), jnp.float32)], axis=0).T


def weighted(got_ref, scale, r):
    acc = scale[r : r + 8, 0:1] * got_ref[0, r : r + 8, :].astype(jnp.float32)
    for j in range(1, got_ref.shape[0]):
        acc = acc + scale[r : r + 8, j : j + 1] * got_ref[j, r : r + 8, :].astype(jnp.float32)
    return acc


def merge_first(got_ref, out_ref):
    peers = got_ref.shape[0]
    row = tails(got_ref)
    top = row(ROW_M) + row(ROW_M + 1)
    part = row(ROW_L) + row(ROW_L + 1)
    snew = row(ROW_S) + row(ROW_S + 1)
    peak = jnp.max(jnp.maximum(top, snew), axis=0, keepdims=True)
    factor = jnp.exp(top - peak)
    fresh = jnp.sum(jnp.where(snew > 0.5 * NEG, jnp.exp(snew - peak), 0.0), axis=0, keepdims=True)
    total = jnp.sum(part * factor, axis=0, keepdims=True) + fresh
    scale = columns([factor, jnp.broadcast_to(fresh, (8, 128))])
    nk, nv = row(ROW_NK), row(ROW_NV)
    accs = []
    for r in range(0, ROW_M, 8):
        accs.append(weighted(got_ref, scale, r) + scale[r : r + 8, peers : peers + 1] * nv)
    tail = jnp.concatenate(
        [*two_pieces(peak), *two_pieces(total), jnp.zeros((4, 128), jnp.float32)], axis=0
    )
    packed = jnp.concatenate(accs + [tail, nk, nv], axis=0).astype(jnp.bfloat16)
    for j in range(out_ref.shape[0]):
        out_ref[j] = packed


def merge_last(got_ref, lam_ref, gain_ref, wo_ref, part_ref, nk_out, nv_out, nk_ref, nv_ref, head_scr, sems):
    seqs = nk_ref.shape[0]
    for h in range(8):
        for dst, r in ((nk_ref, ROW_NKS), (nv_ref, ROW_NVS)):
            dst[:, h * 128 : (h + 1) * 128] = jnp.concatenate(
                [got_ref[b, r : r + 8, :].astype(jnp.float32)[h : h + 1] for b in range(seqs)], axis=0
            ).astype(jnp.bfloat16)
    copies = [
        pltpu.make_async_copy(nk_ref, nk_out, sems.at[0]),
        pltpu.make_async_copy(nv_ref, nv_out, sems.at[1]),
    ]
    for c in copies:
        c.start()
    row = tails(got_ref)
    top = row(ROW_M) + row(ROW_M + 1)
    part = row(ROW_L) + row(ROW_L + 1)
    factor = jnp.exp(top - jnp.max(top, axis=0, keepdims=True))
    total = jnp.sum(part * factor, axis=0, keepdims=True)
    scale = columns([factor / total])
    sub = lax.broadcasted_iota(jnp.int32, (8, 128), 0)
    lam = jnp.zeros((8, 128), jnp.float32)
    for h in range(8):
        lam = jnp.where(sub == h, lam_ref[h], lam)
    for b in range(seqs):
        mixed = weighted(got_ref, scale, b * 16) - lam * weighted(got_ref, scale, b * 16 + 8)
        mean = jnp.mean(mixed * mixed, axis=1, keepdims=True)
        head_scr[b * 8 : b * 8 + 8, :] = mixed * lax.rsqrt(mean + EPS) * gain_ref[...]
    heads = jnp.concatenate(
        [head_scr[pl.ds(h, seqs, stride=8), :] for h in range(8)], axis=1
    ).astype(jnp.bfloat16)
    part_ref[...] = lax.dot_general(
        heads, wo_ref[...], (((1,), (1,)), ((), ())), preferred_element_type=jnp.float32
    ).astype(jnp.bfloat16)
    for c in copies:
        c.wait()


VM = pl.BlockSpec(memory_space=pltpu.VMEM)
SM = pl.BlockSpec(memory_space=pltpu.SMEM)


KV = ("kv_0", "kv_1")


def exchange(array, axis):
    return lax.all_to_all(array, axis, split_axis=0, concat_axis=0, tiled=True)


def per_device(
    tokens, norm_gain, w_query, w_key, w_value, w_output, key_cache, value_cache, lengths, lam, head_gain
):
    peers = lax.axis_size(KV)
    seqs, span, heads, width = key_cache.shape
    sent = pl.pallas_call(
        project,
        out_shape=jax.ShapeDtypeStruct((peers, ROWS_A, 128), jnp.int16),
        in_specs=[pl.BlockSpec(memory_space=pltpu.HBM)] * 5,
        out_specs=VM,
        scratch_shapes=[
            pltpu.VMEM(tokens.shape, jnp.bfloat16),
            pltpu.VMEM((1, norm_gain.shape[0]), jnp.float32),
            pltpu.VMEM(w_query.shape, jnp.bfloat16),
            pltpu.VMEM(w_query.shape, jnp.bfloat16),
            pltpu.VMEM(w_query.shape, jnp.bfloat16),
            pltpu.SemaphoreType.DMA((5,)),
        ],
        name="project",
        cost_estimate=pl.CostEstimate(flops=5_000_000_000, bytes_accessed=30_000_000, transcendentals=0),
        compiler_params=pltpu.CompilerParams(vmem_limit_bytes=8 << 20),
    )(*(pltpu.with_memory_space_constraint(a, pltpu.HBM) for a in (tokens, norm_gain.reshape(1, -1), w_query, w_key, w_value)))
    got = exchange(sent, KV)
    sent = pl.pallas_call(
        attend,
        out_shape=jax.ShapeDtypeStruct((lax.axis_size("kv_0"), ROWS_C, 128), jnp.bfloat16),
        in_specs=[VM, VM, VM, SM],
        out_specs=VM,
        scratch_shapes=[
            pltpu.VMEM((32, 128), jnp.float32),
            pltpu.VMEM((64, 128), jnp.float32),
        ],
        name="attend",
        compiler_params=pltpu.CompilerParams(vmem_limit_bytes=24 << 20),
    )(
        got,
        key_cache.reshape(seqs, span * heads, width),
        value_cache.reshape(seqs, span * heads, width),
        lengths,
    )
    got = exchange(sent, "kv_0")
    sent = pl.pallas_call(
        merge_first,
        out_shape=jax.ShapeDtypeStruct((lax.axis_size("kv_1"), ROWS_E, 128), jnp.bfloat16),
        in_specs=[VM],
        out_specs=VM,
        name="merge_first",
        compiler_params=pltpu.CompilerParams(vmem_limit_bytes=8 << 20),
    )(got)
    got = exchange(sent, "kv_1")
    row = jax.ShapeDtypeStruct((seqs, heads * width), jnp.bfloat16)
    part, new_key, new_value = pl.pallas_call(
        merge_last,
        out_shape=(jax.ShapeDtypeStruct((seqs, w_output.shape[1]), jnp.bfloat16), row, row),
        in_specs=[VM, SM, VM, VM],
        out_specs=(VM, pl.BlockSpec(memory_space=pltpu.HBM), pl.BlockSpec(memory_space=pltpu.HBM)),
        scratch_shapes=[
            pltpu.VMEM(row.shape, row.dtype),
            pltpu.VMEM(row.shape, row.dtype),
            pltpu.VMEM((32, 128), jnp.float32),
            pltpu.SemaphoreType.DMA((2,)),
        ],
        name="merge_last",
        compiler_params=pltpu.CompilerParams(vmem_limit_bytes=8 << 20),
    )(got, lam, head_gain.reshape(1, -1), w_output.T)
    both = lax.all_gather(part, "tp")
    attended = jnp.sum(both.astype(jnp.float32), axis=0).astype(jnp.bfloat16)
    return (attended, new_key, new_value)


def solution(mesh):
    split = Mesh(
        mesh.devices.reshape(mesh.shape["dp"], 8, 4, mesh.shape["tp"]), ("dp", "kv_0", "kv_1", "tp")
    )
    return jax.shard_map(
        per_device,
        mesh=split,
        in_specs=(
            P("dp", KV),
            P(KV),
            P(KV, "tp"),
            P(KV, "tp"),
            P(KV, "tp"),
            P("tp", KV),
            P("dp", KV, "tp", None),
            P("dp", KV, "tp", None),
            P("dp"),
            P("tp"),
            P(),
        ),
        out_specs=(P("dp", KV), P("dp", "tp"), P("dp", "tp")),
        check_vma=False,
    )
```

```python
import jax
import jax.numpy as jnp
from jax import lax
from jax.experimental import pallas as pl
from jax.experimental.pallas import tpu as pltpu
from jax.sharding import Mesh
from jax.sharding import PartitionSpec as P

D = 2048
HEAD_WIDTH = 64
EPS = 1e-6
NEG = -1e30

ROWS_A, BITS = 40, 14.5
ROW_M, ROW_L, ROW_S, ROW_NK, ROW_NV, ROWS_C = 64, 66, 68, 70, 71, 72
ROW_NKS, ROW_NVS, ROWS_E = 72, 80, 88

def exponent(a):
    return jnp.ceil(jnp.log2(jnp.maximum(a, 1e-30)))


def project(tok_hbm, gain_hbm, wq_hbm, wk_hbm, wv_hbm, out_ref, tok_ref, gain_ref, wq_ref, wk_ref, wv_ref, sems):
    copies = [
        pltpu.make_async_copy(src, dst, sems.at[i])
        for i, (src, dst) in enumerate(
            [(tok_hbm, tok_ref), (gain_hbm, gain_ref), (wq_hbm, wq_ref), (wk_hbm, wk_ref), (wv_hbm, wv_ref)]
        )
    ]
    for c in copies:
        c.start()
    for c in copies:
        c.wait()
    peers = out_ref.shape[0]
    x = tok_ref[...].astype(jnp.float32)
    seqs = x.shape[0]
    squares = jnp.sum(x * x, axis=-1, keepdims=True)
    scaled = (x * gain_ref[...]).astype(jnp.bfloat16)
    heads = wq_ref.shape[1] // 128

    def rows(w_ref):
        y = jnp.dot(scaled, w_ref[...], preferred_element_type=jnp.float32)
        e = exponent(jnp.max(jnp.abs(y), axis=1, keepdims=True))
        y = jnp.round(y * jnp.exp2(BITS - e))
        return jnp.concatenate([y[:, h * 128 : (h + 1) * 128] for h in range(heads)], axis=0), e

    (q, qe), (k, ke), (v, ve) = rows(wq_ref), rows(wk_ref), rows(wv_ref)
    se = exponent(squares)
    size = squares * jnp.exp2(BITS - se)
    whole = jnp.floor(size)
    rest = jnp.round((size - whole) * 2.0**14)
    lane = lax.broadcasted_iota(jnp.int32, (seqs, 128), 1)
    meta = jnp.where(
        lane == 0, qe, jnp.where(lane == 1, se, jnp.where(lane == 2, whole, rest))
    )
    q = q.astype(jnp.int32).astype(jnp.int16)
    for j in range(peers):
        b = j % seqs
        tile = jnp.concatenate(
            [
                k[j : j + 1],
                v[j : j + 1],
                jnp.broadcast_to(ke[b : b + 1], (1, 128)),
                jnp.broadcast_to(ve[b : b + 1], (1, 128)),
                meta,
            ],
            axis=0,
        )
        out_ref[j, 0:32, :] = q
        out_ref[j, 32:40, :] = tile.astype(jnp.int32).astype(jnp.int16)


def two_pieces(a):
    hi = a.astype(jnp.bfloat16).astype(jnp.float32)
    return hi, (a - hi).astype(jnp.bfloat16).astype(jnp.float32)


def attend(got_ref, key_ref, val_ref, len_ref, out_ref, q_scr, col_scr):
    peers = got_ref.shape[0]
    seqs = key_ref.shape[0]
    width = key_ref.shape[1]
    span = width // 8
    me = lax.axis_index("kv_0") * lax.axis_size("kv_1") + lax.axis_index("kv_1")
    total = [jnp.zeros((8, 128), jnp.float32)] * 4
    own = jnp.zeros((8, 128), jnp.float32)
    squares = jnp.zeros((8, 128), jnp.float32)
    for j in range(peers):
        got = got_ref[j].astype(jnp.int32).astype(jnp.float32)
        tile = got[32:40]
        unit = jnp.exp2(tile - BITS)
        units = jnp.concatenate([unit[4:8, 0:1]] * 2, axis=0)
        total = [t + got[i * 8 : i * 8 + 8] * units for i, t in enumerate(total)]
        own = own + tile * pltpu.roll(unit, 6, 0)
        size = tile + pltpu.roll(tile, 127, 1) * 2.0**-14
        squares = squares + size * pltpu.roll(unit, 1, 1)
    total = jnp.concatenate(total, axis=0)
    inv = lax.rsqrt(jnp.broadcast_to(squares[4:8, 2:3], (4, 128)) / D + EPS)
    inv8 = jnp.concatenate([inv, inv], axis=0)
    inv32 = jnp.concatenate([inv8] * 4, axis=0)
    q = (total * inv32).astype(jnp.bfloat16).astype(jnp.float32)
    q_scr[...] = q
    seq_id = lax.broadcasted_iota(jnp.int32, (seqs, 128), 0)
    mine = jnp.sum(jnp.where(seq_id == lax.rem(me, seqs), inv, 0.0), axis=0, keepdims=True)
    nk = (own[0:1] * mine).astype(jnp.bfloat16)
    nv = (own[1:2] * mine).astype(jnp.bfloat16)
    lane = lax.broadcasted_iota(jnp.int32, (8, 128), 1)
    sub = lax.broadcasted_iota(jnp.int32, (8, 128), 0)
    lane1 = lax.broadcasted_iota(jnp.int32, (1, 128), 1)
    qk = q_scr[pl.ds(me, 1), :] * nk.astype(jnp.float32) * HEAD_WIDTH**-0.5
    s1 = jnp.sum(jnp.where(lane1 < HEAD_WIDTH, qk, 0.0), axis=1, keepdims=True)
    s2 = jnp.sum(jnp.where(lane1 >= HEAD_WIDTH, qk, 0.0), axis=1, keepdims=True)
    spot = lax.rem(me, seqs) * 16 + me // seqs
    snew = jnp.where(lane1 == spot, s1, jnp.where(lane1 == spot + 8, s2, NEG))
    own_head = lax.rem(lane, 8) == sub
    col = lax.broadcasted_iota(jnp.int32, (8, width), 1)
    own_head_wide = lax.rem(col, 8) == lax.broadcasted_iota(jnp.int32, (8, width), 0)

    def score(b):
        qb = q_scr[pl.ds(b, 8, stride=seqs), :] * HEAD_WIDTH**-0.5
        q1 = jnp.where(lane < HEAD_WIDTH, qb, 0.0)
        q2 = jnp.where(lane >= HEAD_WIDTH, qb, 0.0)
        q16 = jnp.concatenate([q1, q2], axis=0).astype(jnp.bfloat16)
        return lax.dot_general(
            q16, key_ref[b], (((1,), (1,)), ((), ())), preferred_element_type=jnp.float32
        )

    def weigh(b, s):
        limit = (len_ref[b] - me * span) * 8
        live = jnp.logical_and(own_head_wide, col < limit)
        weights = []
        for m in range(2):
            part = jnp.where(live, s[m * 8 : (m + 1) * 8], NEG)
            hi, lo = two_pieces(jnp.max(part, axis=1, keepdims=True))
            w = jnp.where(live, jnp.exp(part - (hi + lo)), 0.0)
            lhi, llo = two_pieces(jnp.sum(w, axis=1, keepdims=True))
            weights.append(w)
            r = b * 16 + m * 8
            col_scr[r : r + 8, :] = jnp.where(
                lane == 0, hi, jnp.where(lane == 1, lo, jnp.where(lane == 2, lhi, llo))
            )
        return jnp.concatenate(weights, axis=0).astype(jnp.bfloat16)

    def values(b, w):
        return jnp.dot(w, val_ref[b], preferred_element_type=jnp.float32)

    scores = [score(b) for b in range(seqs)]
    weights = [weigh(b, scores[b]) for b in range(seqs)]
    accs = [values(b, weights[b]) for b in range(seqs)]
    turned = jnp.concatenate([col_scr[...], jnp.zeros_like(col_scr)], axis=0).T
    shi, slo = two_pieces(snew)
    tail = jnp.concatenate(
        [turned[0:4], shi, slo, nk.astype(jnp.float32), nv.astype(jnp.float32)], axis=0
    )
    packed = jnp.concatenate(accs + [tail], axis=0).astype(jnp.bfloat16)
    for j in range(out_ref.shape[0]):
        out_ref[j] = packed


def tails(got_ref):
    peers = got_ref.shape[0]
    tiles = [got_ref[j, ROW_M : ROW_M + 8, :].astype(jnp.float32) for j in range(peers)]
    return lambda r: jnp.concatenate([t[r - ROW_M : r - ROW_M + 1] for t in tiles], axis=0)


def columns(rows):
    used = sum(r.shape[0] for r in rows)
    return jnp.concatenate(rows + [jnp.zeros((128 - used, 128), jnp.float32)], axis=0).T


def weighted(got_ref, scale, r):
    acc = scale[r : r + 8, 0:1] * got_ref[0, r : r + 8, :].astype(jnp.float32)
    for j in range(1, got_ref.shape[0]):
        acc = acc + scale[r : r + 8, j : j + 1] * got_ref[j, r : r + 8, :].astype(jnp.float32)
    return acc


def merge_first(got_ref, out_ref):
    peers = got_ref.shape[0]
    row = tails(got_ref)
    top = row(ROW_M) + row(ROW_M + 1)
    part = row(ROW_L) + row(ROW_L + 1)
    snew = row(ROW_S) + row(ROW_S + 1)
    peak = jnp.max(jnp.maximum(top, snew), axis=0, keepdims=True)
    factor = jnp.exp(top - peak)
    fresh = jnp.sum(jnp.where(snew > 0.5 * NEG, jnp.exp(snew - peak), 0.0), axis=0, keepdims=True)
    total = jnp.sum(part * factor, axis=0, keepdims=True) + fresh
    scale = columns([factor, jnp.broadcast_to(fresh, (8, 128))])
    nk, nv = row(ROW_NK), row(ROW_NV)
    accs = []
    for r in range(0, ROW_M, 8):
        accs.append(weighted(got_ref, scale, r) + scale[r : r + 8, peers : peers + 1] * nv)
    tail = jnp.concatenate(
        [*two_pieces(peak), *two_pieces(total), jnp.zeros((4, 128), jnp.float32)], axis=0
    )
    packed = jnp.concatenate(accs + [tail, nk, nv], axis=0).astype(jnp.bfloat16)
    for j in range(out_ref.shape[0]):
        out_ref[j] = packed


def by_seq(scr, seqs):
    rows = [scr[pl.ds(h, seqs, stride=8), :] for h in range(8)]
    return jnp.concatenate(rows, axis=1).astype(jnp.bfloat16)


def merge_last(got_ref, lam_ref, gain_ref, wo_ref, part_ref, nk_ref, nv_ref, head_scr):
    seqs = nk_ref.shape[0]
    for dst, r in ((nk_ref, ROW_NKS), (nv_ref, ROW_NVS)):
        for b in range(seqs):
            head_scr[b * 8 : b * 8 + 8, :] = got_ref[b, r : r + 8, :].astype(jnp.float32)
        dst[...] = by_seq(head_scr, seqs)
    row = tails(got_ref)
    top = row(ROW_M) + row(ROW_M + 1)
    part = row(ROW_L) + row(ROW_L + 1)
    factor = jnp.exp(top - jnp.max(top, axis=0, keepdims=True))
    total = jnp.sum(part * factor, axis=0, keepdims=True)
    scale = columns([factor / total])
    sub = lax.broadcasted_iota(jnp.int32, (8, 128), 0)
    lam = jnp.zeros((8, 128), jnp.float32)
    for h in range(8):
        lam = jnp.where(sub == h, lam_ref[h], lam)
    for b in range(seqs):
        mixed = weighted(got_ref, scale, b * 16) - lam * weighted(got_ref, scale, b * 16 + 8)
        mean = jnp.mean(mixed * mixed, axis=1, keepdims=True)
        head_scr[b * 8 : b * 8 + 8, :] = mixed * lax.rsqrt(mean + EPS) * gain_ref[...]
    heads = by_seq(head_scr, seqs)
    part_ref[...] = lax.dot_general(
        heads, wo_ref[...], (((1,), (1,)), ((), ())), preferred_element_type=jnp.float32
    ).astype(jnp.bfloat16)


def finish(both_ref, nk_ref, nv_ref, out, nk_out, nv_out, sum_ref, sems):
    copies = [
        pltpu.make_async_copy(src, dst, sems.at[i])
        for i, (src, dst) in enumerate(((nk_ref, nk_out), (nv_ref, nv_out), (sum_ref, out)))
    ]
    copies[0].start()
    copies[1].start()
    total = both_ref[0].astype(jnp.float32) + both_ref[1].astype(jnp.float32)
    sum_ref[...] = total.astype(sum_ref.dtype)
    copies[2].start()
    for c in copies:
        c.wait()


HB = pl.BlockSpec(memory_space=pltpu.HBM)
VM = pl.BlockSpec(memory_space=pltpu.VMEM)
SM = pl.BlockSpec(memory_space=pltpu.SMEM)


KV = ("kv_0", "kv_1")


def exchange(array, axis):
    return lax.all_to_all(array, axis, split_axis=0, concat_axis=0, tiled=True)


def per_device(
    tokens, norm_gain, w_query, w_key, w_value, w_output, key_cache, value_cache, lengths, lam, head_gain
):
    peers = lax.axis_size(KV)
    seqs, span, heads, width = key_cache.shape
    sent = pl.pallas_call(
        project,
        out_shape=jax.ShapeDtypeStruct((peers, ROWS_A, 128), jnp.int16),
        in_specs=[pl.BlockSpec(memory_space=pltpu.HBM)] * 5,
        out_specs=VM,
        scratch_shapes=[
            pltpu.VMEM(tokens.shape, jnp.bfloat16),
            pltpu.VMEM((1, norm_gain.shape[0]), jnp.float32),
            pltpu.VMEM(w_query.shape, jnp.bfloat16),
            pltpu.VMEM(w_query.shape, jnp.bfloat16),
            pltpu.VMEM(w_query.shape, jnp.bfloat16),
            pltpu.SemaphoreType.DMA((5,)),
        ],
        name="project",
        cost_estimate=pl.CostEstimate(flops=5_000_000_000, bytes_accessed=30_000_000, transcendentals=0),
        compiler_params=pltpu.CompilerParams(vmem_limit_bytes=8 << 20),
    )(*(pltpu.with_memory_space_constraint(a, pltpu.HBM) for a in (tokens, norm_gain.reshape(1, -1), w_query, w_key, w_value)))
    got = exchange(sent, KV)
    sent = pl.pallas_call(
        attend,
        out_shape=jax.ShapeDtypeStruct((lax.axis_size("kv_0"), ROWS_C, 128), jnp.bfloat16),
        in_specs=[VM, VM, VM, SM],
        out_specs=VM,
        scratch_shapes=[
            pltpu.VMEM((32, 128), jnp.float32),
            pltpu.VMEM((64, 128), jnp.float32),
        ],
        name="attend",
        compiler_params=pltpu.CompilerParams(vmem_limit_bytes=24 << 20),
    )(
        got,
        key_cache.reshape(seqs, span * heads, width),
        value_cache.reshape(seqs, span * heads, width),
        lengths,
    )
    got = exchange(sent, "kv_0")
    sent = pl.pallas_call(
        merge_first,
        out_shape=jax.ShapeDtypeStruct((lax.axis_size("kv_1"), ROWS_E, 128), jnp.bfloat16),
        in_specs=[VM],
        out_specs=VM,
        name="merge_first",
        compiler_params=pltpu.CompilerParams(vmem_limit_bytes=8 << 20),
    )(got)
    got = exchange(sent, "kv_1")
    row = jax.ShapeDtypeStruct((seqs, heads * width), jnp.bfloat16)
    part, new_key, new_value = pl.pallas_call(
        merge_last,
        out_shape=(jax.ShapeDtypeStruct((seqs, w_output.shape[1]), jnp.bfloat16),) + (pltpu.VMEM(row.shape, row.dtype),) * 2,
        in_specs=[VM, SM, VM, VM],
        out_specs=(VM, VM, VM),
        scratch_shapes=[
            pltpu.VMEM((32, 128), jnp.float32),
        ],
        name="merge_last",
        compiler_params=pltpu.CompilerParams(vmem_limit_bytes=8 << 20),
    )(got, lam, head_gain.reshape(1, -1), w_output.T)
    both = lax.all_gather(part, "tp")
    attended, new_key, new_value = pl.pallas_call(
        finish,
        out_shape=(jax.ShapeDtypeStruct(part.shape, part.dtype), row, row),
        in_specs=[VM] * 3,
        out_specs=(HB, HB, HB),
        scratch_shapes=[pltpu.VMEM(part.shape, part.dtype), pltpu.SemaphoreType.DMA((3,))],
        name="finish",
        compiler_params=pltpu.CompilerParams(vmem_limit_bytes=8 << 20),
    )(both, new_key, new_value)
    return (attended, new_key, new_value)


def solution(mesh):
    split = Mesh(
        mesh.devices.reshape(mesh.shape["dp"], 8, 4, mesh.shape["tp"]), ("dp", "kv_0", "kv_1", "tp")
    )
    return jax.shard_map(
        per_device,
        mesh=split,
        in_specs=(
            P("dp", KV),
            P(KV),
            P(KV, "tp"),
            P(KV, "tp"),
            P(KV, "tp"),
            P("tp", KV),
            P("dp", KV, "tp", None),
            P("dp", KV, "tp", None),
            P("dp"),
            P("tp"),
            P(),
        ),
        out_specs=(P("dp", KV), P("dp", "tp"), P("dp", "tp")),
        check_vma=False,
    )
```

```python
import jax
import jax.numpy as jnp
from jax import lax
from jax.experimental import pallas as pl
from jax.experimental.pallas import tpu as pltpu
from jax.sharding import Mesh
from jax.sharding import PartitionSpec as P

D = 2048
HEAD_WIDTH = 64
EPS = 1e-6
NEG = -1e30

BITS = 14.5
ROW_M, ROW_L, ROW_S, ROW_NK, ROW_NV, ROWS_C = 64, 66, 68, 70, 71, 72
ROW_NKS, ROW_NVS, ROWS_E = 72, 80, 88

def exponent(a):
    return jnp.ceil(jnp.log2(jnp.maximum(a, 1e-30)))


def project(tok_hbm, gain_hbm, wq_hbm, wk_hbm, wv_hbm, out_ref, tok_ref, gain_ref, wq_ref, wk_ref, wv_ref, sems):
    copies = [
        pltpu.make_async_copy(src, dst, sems.at[i])
        for i, (src, dst) in enumerate(
            [(tok_hbm, tok_ref), (gain_hbm, gain_ref), (wq_hbm, wq_ref), (wk_hbm, wk_ref), (wv_hbm, wv_ref)]
        )
    ]
    for c in copies:
        c.start()
    for c in copies:
        c.wait()
    peers = out_ref.shape[0]
    x = tok_ref[...].astype(jnp.float32)
    seqs = x.shape[0]
    squares = jnp.sum(x * x, axis=-1, keepdims=True)
    scaled = (x * gain_ref[...]).astype(jnp.bfloat16)
    heads = wq_ref.shape[1] // 128

    def rows(w_ref):
        y = jnp.dot(scaled, w_ref[...], preferred_element_type=jnp.float32)
        e = exponent(jnp.max(jnp.abs(y), axis=1, keepdims=True))
        y = jnp.round(y * jnp.exp2(BITS - e))
        return jnp.concatenate([y[:, h * 128 : (h + 1) * 128] for h in range(heads)], axis=0), e

    (q, qe), (k, ke), (v, ve) = rows(wq_ref), rows(wk_ref), rows(wv_ref)
    se = exponent(squares)
    size = squares * jnp.exp2(BITS - se)
    whole = jnp.floor(size)
    rest = jnp.round((size - whole) * 2.0**14)
    lane = lax.broadcasted_iota(jnp.int32, (seqs, 128), 1)
    sub = lax.broadcasted_iota(jnp.int32, (seqs, 128), 0)
    meta = jnp.where(
        lane == 0, qe, jnp.where(lane == 1, se, jnp.where(lane == 2, whole, rest))
    )
    metas = [
        jnp.where(lane == 4, jnp.where(sub < 2, ke[b : b + 1], ve[b : b + 1]), meta)
        for b in range(seqs)
    ]
    q = q.astype(jnp.int32).astype(jnp.int16)
    kr, vr = pltpu.roll(k, 64, 1), pltpu.roll(v, 64, 1)
    for j in range(peers):
        tile = jnp.concatenate([kr[j : j + 1], k[j : j + 1], vr[j : j + 1], v[j : j + 1]], axis=0)
        tile = jnp.where(lane < 64, metas[j % seqs], tile)
        for h in range(heads):
            out_ref[j, h] = q[h * seqs : (h + 1) * seqs]
        out_ref[j, heads] = tile.astype(jnp.int32).astype(jnp.int16)


def two_pieces(a):
    hi = a.astype(jnp.bfloat16).astype(jnp.float32)
    return hi, (a - hi).astype(jnp.bfloat16).astype(jnp.float32)


def attend(got_ref, key_ref, val_ref, len_ref, out_ref, q_scr, col_scr):
    peers = got_ref.shape[0]
    seqs = key_ref.shape[0]
    width = key_ref.shape[1]
    span = width // 8
    me = lax.axis_index("kv_0") * lax.axis_size("kv_1") + lax.axis_index("kv_1")
    total = [jnp.zeros((seqs, 128), jnp.float32)] * 8
    own = jnp.zeros((seqs, 128), jnp.float32)
    squares = jnp.zeros((seqs, 128), jnp.float32)
    for j in range(peers):
        got = [got_ref[j, i].astype(jnp.int32).astype(jnp.float32) for i in range(9)]
        tile = got[8]
        unit = jnp.exp2(tile - BITS)
        total = [t + g * unit[:, 0:1] for t, g in zip(total, got)]
        own = own + tile * unit[:, 4:5]
        size = tile + pltpu.roll(tile, 127, 1) * 2.0**-14
        squares = squares + size * pltpu.roll(unit, 1, 1)
    lane1 = lax.broadcasted_iota(jnp.int32, (1, 128), 1)
    swap = pltpu.roll(own, 64, 1)
    own_k = jnp.where(lane1 < 64, swap[0:1], own[1:2])
    own_v = jnp.where(lane1 < 64, swap[2:3], own[3:4])
    total = jnp.concatenate(total, axis=0)
    inv = lax.rsqrt(jnp.broadcast_to(squares[:, 2:3], (seqs, 128)) / D + EPS)
    inv8 = jnp.concatenate([inv, inv], axis=0)
    inv32 = jnp.concatenate([inv8] * 4, axis=0)
    q = (total * inv32).astype(jnp.bfloat16).astype(jnp.float32)
    q_scr[...] = q
    seq_id = lax.broadcasted_iota(jnp.int32, (seqs, 128), 0)
    mine = jnp.sum(jnp.where(seq_id == lax.rem(me, seqs), inv, 0.0), axis=0, keepdims=True)
    nk = (own_k * mine).astype(jnp.bfloat16)
    nv = (own_v * mine).astype(jnp.bfloat16)
    lane = lax.broadcasted_iota(jnp.int32, (8, 128), 1)
    sub = lax.broadcasted_iota(jnp.int32, (8, 128), 0)
    lane1 = lax.broadcasted_iota(jnp.int32, (1, 128), 1)
    qk = q_scr[pl.ds(me, 1), :] * nk.astype(jnp.float32) * HEAD_WIDTH**-0.5
    s1 = jnp.sum(jnp.where(lane1 < HEAD_WIDTH, qk, 0.0), axis=1, keepdims=True)
    s2 = jnp.sum(jnp.where(lane1 >= HEAD_WIDTH, qk, 0.0), axis=1, keepdims=True)
    spot = lax.rem(me, seqs) * 16 + me // seqs
    snew = jnp.where(lane1 == spot, s1, jnp.where(lane1 == spot + 8, s2, NEG))
    own_head = lax.rem(lane, 8) == sub
    col = lax.broadcasted_iota(jnp.int32, (8, width), 1)
    own_head_wide = lax.rem(col, 8) == lax.broadcasted_iota(jnp.int32, (8, width), 0)
    col = col.astype(jnp.float32)
    lane4 = lax.broadcasted_iota(jnp.int32, (1, seqs), 1)
    ends = ((len_ref[...] - me * span) * 8).astype(jnp.float32)

    def score(b):
        qb = q_scr[pl.ds(b, 8, stride=seqs), :] * HEAD_WIDTH**-0.5
        q1 = jnp.where(lane < HEAD_WIDTH, qb, 0.0)
        q2 = jnp.where(lane >= HEAD_WIDTH, qb, 0.0)
        q16 = jnp.concatenate([q1, q2], axis=0).astype(jnp.bfloat16)
        return lax.dot_general(
            q16, key_ref[b], (((1,), (1,)), ((), ())), preferred_element_type=jnp.float32
        )

    def weigh(b, s):
        limit = jnp.sum(jnp.where(lane4 == b, ends, 0.0), axis=1, keepdims=True)
        live = jnp.logical_and(own_head_wide, col < limit)
        weights = []
        for m in range(2):
            part = jnp.where(live, s[m * 8 : (m + 1) * 8], NEG)
            hi, lo = two_pieces(jnp.max(part, axis=1, keepdims=True))
            w = jnp.where(live, jnp.exp(part - (hi + lo)), 0.0)
            lhi, llo = two_pieces(jnp.sum(w, axis=1, keepdims=True))
            weights.append(w)
            r = b * 16 + m * 8
            col_scr[r : r + 8, :] = jnp.where(
                lane == 0, hi, jnp.where(lane == 1, lo, jnp.where(lane == 2, lhi, llo))
            )
        return jnp.concatenate(weights, axis=0).astype(jnp.bfloat16)

    def values(b, w):
        return jnp.dot(w, val_ref[b], preferred_element_type=jnp.float32)

    scores = [score(b) for b in range(seqs)]
    weights = [weigh(b, scores[b]) for b in range(seqs)]
    accs = [values(b, weights[b]) for b in range(seqs)]
    turned = jnp.concatenate([col_scr[...], jnp.zeros_like(col_scr)], axis=0).T
    shi, slo = two_pieces(snew)
    tail = jnp.concatenate(
        [turned[0:4], shi, slo, nk.astype(jnp.float32), nv.astype(jnp.float32)], axis=0
    )
    packed = jnp.concatenate(accs + [tail], axis=0).astype(jnp.bfloat16)
    for j in range(out_ref.shape[0]):
        out_ref[j] = packed


def tails(got_ref):
    peers = got_ref.shape[0]
    tiles = [got_ref[j, ROW_M : ROW_M + 8, :].astype(jnp.float32) for j in range(peers)]
    return lambda r: jnp.concatenate([t[r - ROW_M : r - ROW_M + 1] for t in tiles], axis=0)


def columns(rows):
    used = sum(r.shape[0] for r in rows)
    return jnp.concatenate(rows + [jnp.zeros((128 - used, 128), jnp.float32)], axis=0).T


def weighted(got_ref, scale, r):
    acc = scale[r : r + 8, 0:1] * got_ref[0, r : r + 8, :].astype(jnp.float32)
    for j in range(1, got_ref.shape[0]):
        acc = acc + scale[r : r + 8, j : j + 1] * got_ref[j, r : r + 8, :].astype(jnp.float32)
    return acc


def merge_first(got_ref, out_ref):
    peers = got_ref.shape[0]
    row = tails(got_ref)
    top = row(ROW_M) + row(ROW_M + 1)
    part = row(ROW_L) + row(ROW_L + 1)
    snew = row(ROW_S) + row(ROW_S + 1)
    peak = jnp.max(jnp.maximum(top, snew), axis=0, keepdims=True)
    factor = jnp.exp(top - peak)
    fresh = jnp.sum(jnp.where(snew > 0.5 * NEG, jnp.exp(snew - peak), 0.0), axis=0, keepdims=True)
    total = jnp.sum(part * factor, axis=0, keepdims=True) + fresh
    scale = columns([factor, jnp.broadcast_to(fresh, (8, 128))])
    nk, nv = row(ROW_NK), row(ROW_NV)
    accs = []
    for r in range(0, ROW_M, 8):
        accs.append(weighted(got_ref, scale, r) + scale[r : r + 8, peers : peers + 1] * nv)
    tail = jnp.concatenate(
        [*two_pieces(peak), *two_pieces(total), jnp.zeros((4, 128), jnp.float32)], axis=0
    )
    packed = jnp.concatenate(accs + [tail, nk, nv], axis=0).astype(jnp.bfloat16)
    for j in range(out_ref.shape[0]):
        out_ref[j] = packed


def by_seq(scr, seqs):
    rows = [scr[pl.ds(h, seqs, stride=8), :] for h in range(8)]
    return jnp.concatenate(rows, axis=1).astype(jnp.bfloat16)


def merge_last(got_ref, lam_ref, gain_ref, wo_ref, part_ref, nk_ref, nv_ref, head_scr):
    seqs = nk_ref.shape[0]
    for dst, r in ((nk_ref, ROW_NKS), (nv_ref, ROW_NVS)):
        for b in range(seqs):
            head_scr[b * 8 : b * 8 + 8, :] = got_ref[b, r : r + 8, :].astype(jnp.float32)
        dst[...] = by_seq(head_scr, seqs)
    row = tails(got_ref)
    top = row(ROW_M) + row(ROW_M + 1)
    part = row(ROW_L) + row(ROW_L + 1)
    factor = jnp.exp(top - jnp.max(top, axis=0, keepdims=True))
    total = jnp.sum(part * factor, axis=0, keepdims=True)
    scale = columns([factor / total])
    lane8 = lax.broadcasted_iota(jnp.int32, (8, 8), 1)
    sub8 = lax.broadcasted_iota(jnp.int32, (8, 8), 0)
    lam = jnp.sum(jnp.where(lane8 == sub8, lam_ref[...], 0.0), axis=1, keepdims=True)
    for b in range(seqs):
        mixed = weighted(got_ref, scale, b * 16) - lam * weighted(got_ref, scale, b * 16 + 8)
        mean = jnp.mean(mixed * mixed, axis=1, keepdims=True)
        head_scr[b * 8 : b * 8 + 8, :] = mixed * lax.rsqrt(mean + EPS) * gain_ref[...]
    heads = by_seq(head_scr, seqs)
    part_ref[...] = lax.dot_general(
        heads, wo_ref[...], (((1,), (1,)), ((), ())), preferred_element_type=jnp.float32
    ).astype(jnp.bfloat16)


def finish(both_ref, nk_ref, nv_ref, out, nk_out, nv_out, sum_ref, sems):
    copies = [
        pltpu.make_async_copy(src, dst, sems.at[i])
        for i, (src, dst) in enumerate(((nk_ref, nk_out), (nv_ref, nv_out), (sum_ref, out)))
    ]
    copies[0].start()
    copies[1].start()
    total = both_ref[0].astype(jnp.float32) + both_ref[1].astype(jnp.float32)
    sum_ref[...] = total.astype(sum_ref.dtype)
    copies[2].start()
    for c in copies:
        c.wait()


HB = pl.BlockSpec(memory_space=pltpu.HBM)
VM = pl.BlockSpec(memory_space=pltpu.VMEM)


KV = ("kv_0", "kv_1")


def exchange(array, axis):
    return lax.all_to_all(array, axis, split_axis=0, concat_axis=0, tiled=True)


def per_device(
    tokens, norm_gain, w_query, w_key, w_value, w_output, key_cache, value_cache, lengths, lam, head_gain
):
    peers = lax.axis_size(KV)
    seqs, span, heads, width = key_cache.shape
    sent = pl.pallas_call(
        project,
        out_shape=jax.ShapeDtypeStruct((peers, heads + 1, seqs, 128), jnp.int16),
        in_specs=[pl.BlockSpec(memory_space=pltpu.HBM)] * 5,
        out_specs=VM,
        scratch_shapes=[
            pltpu.VMEM(tokens.shape, jnp.bfloat16),
            pltpu.VMEM((1, norm_gain.shape[0]), jnp.float32),
            pltpu.VMEM(w_query.shape, jnp.bfloat16),
            pltpu.VMEM(w_query.shape, jnp.bfloat16),
            pltpu.VMEM(w_query.shape, jnp.bfloat16),
            pltpu.SemaphoreType.DMA((5,)),
        ],
        name="project",
        cost_estimate=pl.CostEstimate(flops=5_000_000_000, bytes_accessed=30_000_000, transcendentals=0),
        compiler_params=pltpu.CompilerParams(vmem_limit_bytes=8 << 20),
    )(*(pltpu.with_memory_space_constraint(a, pltpu.HBM) for a in (tokens, norm_gain.reshape(1, -1), w_query, w_key, w_value)))
    got = exchange(sent, KV)
    sent = pl.pallas_call(
        attend,
        out_shape=jax.ShapeDtypeStruct((lax.axis_size("kv_0"), ROWS_C, 128), jnp.bfloat16),
        in_specs=[VM] * 4,
        out_specs=VM,
        scratch_shapes=[
            pltpu.VMEM((32, 128), jnp.float32),
            pltpu.VMEM((64, 128), jnp.float32),
        ],
        name="attend",
        compiler_params=pltpu.CompilerParams(vmem_limit_bytes=24 << 20),
    )(
        got,
        key_cache.reshape(seqs, span * heads, width),
        value_cache.reshape(seqs, span * heads, width),
        lengths.reshape(1, -1),
    )
    got = exchange(sent, "kv_0")
    sent = pl.pallas_call(
        merge_first,
        out_shape=jax.ShapeDtypeStruct((lax.axis_size("kv_1"), ROWS_E, 128), jnp.bfloat16),
        in_specs=[VM],
        out_specs=VM,
        name="merge_first",
        compiler_params=pltpu.CompilerParams(vmem_limit_bytes=8 << 20),
    )(got)
    got = exchange(sent, "kv_1")
    row = jax.ShapeDtypeStruct((seqs, heads * width), jnp.bfloat16)
    part, new_key, new_value = pl.pallas_call(
        merge_last,
        out_shape=(jax.ShapeDtypeStruct((seqs, w_output.shape[1]), jnp.bfloat16),) + (pltpu.VMEM(row.shape, row.dtype),) * 2,
        in_specs=[VM] * 4,
        out_specs=(VM, VM, VM),
        scratch_shapes=[
            pltpu.VMEM((32, 128), jnp.float32),
        ],
        name="merge_last",
        compiler_params=pltpu.CompilerParams(vmem_limit_bytes=8 << 20),
    )(got, lam.reshape(1, -1), head_gain.reshape(1, -1), w_output.T)
    both = lax.all_gather(part, "tp")
    attended, new_key, new_value = pl.pallas_call(
        finish,
        out_shape=(jax.ShapeDtypeStruct(part.shape, part.dtype), row, row),
        in_specs=[VM] * 3,
        out_specs=(HB, HB, HB),
        scratch_shapes=[pltpu.VMEM(part.shape, part.dtype), pltpu.SemaphoreType.DMA((3,))],
        name="finish",
        compiler_params=pltpu.CompilerParams(vmem_limit_bytes=8 << 20),
    )(both, new_key, new_value)
    return (attended, new_key, new_value)


def solution(mesh):
    split = Mesh(
        mesh.devices.reshape(mesh.shape["dp"], 8, 4, mesh.shape["tp"]), ("dp", "kv_0", "kv_1", "tp")
    )
    return jax.shard_map(
        per_device,
        mesh=split,
        in_specs=(
            P("dp", KV),
            P(KV),
            P(KV, "tp"),
            P(KV, "tp"),
            P(KV, "tp"),
            P("tp", KV),
            P("dp", KV, "tp", None),
            P("dp", KV, "tp", None),
            P("dp"),
            P("tp"),
            P(),
        ),
        out_specs=(P("dp", KV), P("dp", "tp"), P("dp", "tp")),
        check_vma=False,
    )
```

```python
import jax
import jax.numpy as jnp
from jax import lax
from jax.experimental import pallas as pl
from jax.experimental.pallas import tpu as pltpu
from jax.sharding import Mesh
from jax.sharding import PartitionSpec as P

D = 2048
HEAD_WIDTH = 64
EPS = 1e-6
NEG = -1e30

BITS = 14.5
ROW_M, ROW_L, ROW_S, ROW_NK, ROW_NV, ROWS_C = 64, 66, 68, 70, 71, 72
ROW_NKS, ROW_NVS, ROWS_E = 72, 80, 88

def exponent(a):
    return jnp.ceil(jnp.log2(jnp.maximum(a, 1e-30)))


def project(tok_hbm, gain_hbm, wq_hbm, wk_hbm, wv_hbm, out_ref, tok_ref, gain_ref, wq_ref, wk_ref, wv_ref, sems):
    copies = [
        pltpu.make_async_copy(src, dst, sems.at[i])
        for i, (src, dst) in enumerate(
            [(tok_hbm, tok_ref), (gain_hbm, gain_ref), (wq_hbm, wq_ref), (wk_hbm, wk_ref), (wv_hbm, wv_ref)]
        )
    ]
    for c in copies:
        c.start()
    for c in copies:
        c.wait()
    peers = out_ref.shape[0]
    x = tok_ref[...].astype(jnp.float32)
    seqs = x.shape[0]
    squares = jnp.sum(x * x, axis=-1, keepdims=True)
    scaled = (x * gain_ref[...]).astype(jnp.bfloat16)
    heads = wq_ref.shape[1] // 128

    def rows(w_ref):
        y = jnp.dot(scaled, w_ref[...], preferred_element_type=jnp.float32)
        e = exponent(jnp.max(jnp.abs(y), axis=1, keepdims=True))
        y = jnp.round(y * jnp.exp2(BITS - e))
        return jnp.concatenate([y[:, h * 128 : (h + 1) * 128] for h in range(heads)], axis=0), e

    (q, qe), (k, ke), (v, ve) = rows(wq_ref), rows(wk_ref), rows(wv_ref)
    se = exponent(squares)
    size = squares * jnp.exp2(BITS - se)
    whole = jnp.floor(size)
    rest = jnp.round((size - whole) * 2.0**14)
    lane = lax.broadcasted_iota(jnp.int32, (seqs, 128), 1)
    sub = lax.broadcasted_iota(jnp.int32, (seqs, 128), 0)
    meta = jnp.where(
        lane == 0, qe, jnp.where(lane == 1, se, jnp.where(lane == 2, whole, rest))
    )
    metas = [
        jnp.where(lane == 4, jnp.where(sub < 2, ke[b : b + 1], ve[b : b + 1]), meta)
        for b in range(seqs)
    ]
    q = q.astype(jnp.int32).astype(jnp.int16)
    kr, vr = pltpu.roll(k, 64, 1), pltpu.roll(v, 64, 1)
    for j in range(peers):
        tile = jnp.concatenate([kr[j : j + 1], k[j : j + 1], vr[j : j + 1], v[j : j + 1]], axis=0)
        tile = jnp.where(lane < 64, metas[j % seqs], tile)
        for h in range(heads):
            out_ref[j, h] = q[h * seqs : (h + 1) * seqs]
        out_ref[j, heads] = tile.astype(jnp.int32).astype(jnp.int16)


def two_pieces(a):
    hi = a.astype(jnp.bfloat16).astype(jnp.float32)
    return hi, (a - hi).astype(jnp.bfloat16).astype(jnp.float32)


def attend(got_ref, key_ref, val_ref, len_ref, out_ref, q_scr, col_scr):
    peers = got_ref.shape[0]
    seqs = key_ref.shape[0]
    width = key_ref.shape[1]
    span = width // 8
    me = lax.axis_index("kv_0") * lax.axis_size("kv_1") + lax.axis_index("kv_1")
    total = [jnp.zeros((seqs, 128), jnp.float32)] * 8
    own = jnp.zeros((seqs, 128), jnp.float32)
    squares = jnp.zeros((seqs, 128), jnp.float32)
    for j in range(peers):
        got = [got_ref[j, i].astype(jnp.int32).astype(jnp.float32) for i in range(9)]
        tile = got[8]
        unit = jnp.exp2(tile - BITS)
        total = [t + g * unit[:, 0:1] for t, g in zip(total, got)]
        own = own + tile * unit[:, 4:5]
        size = tile + pltpu.roll(tile, 127, 1) * 2.0**-14
        squares = squares + size * pltpu.roll(unit, 1, 1)
    lane1 = lax.broadcasted_iota(jnp.int32, (1, 128), 1)
    swap = pltpu.roll(own, 64, 1)
    own_k = jnp.where(lane1 < 64, swap[0:1], own[1:2])
    own_v = jnp.where(lane1 < 64, swap[2:3], own[3:4])
    total = jnp.concatenate(total, axis=0)
    inv = lax.rsqrt(jnp.broadcast_to(squares[:, 2:3], (seqs, 128)) / D + EPS)
    inv8 = jnp.concatenate([inv, inv], axis=0)
    inv32 = jnp.concatenate([inv8] * 4, axis=0)
    q = (total * inv32).astype(jnp.bfloat16).astype(jnp.float32)
    q_scr[...] = q
    seq_id = lax.broadcasted_iota(jnp.int32, (seqs, 128), 0)
    mine = jnp.sum(jnp.where(seq_id == lax.rem(me, seqs), inv, 0.0), axis=0, keepdims=True)
    nk = (own_k * mine).astype(jnp.bfloat16)
    nv = (own_v * mine).astype(jnp.bfloat16)
    lane = lax.broadcasted_iota(jnp.int32, (8, 128), 1)
    sub = lax.broadcasted_iota(jnp.int32, (8, 128), 0)
    lane1 = lax.broadcasted_iota(jnp.int32, (1, 128), 1)
    qk = q_scr[pl.ds(me, 1), :] * nk.astype(jnp.float32) * HEAD_WIDTH**-0.5
    s1 = jnp.sum(jnp.where(lane1 < HEAD_WIDTH, qk, 0.0), axis=1, keepdims=True)
    s2 = jnp.sum(jnp.where(lane1 >= HEAD_WIDTH, qk, 0.0), axis=1, keepdims=True)
    spot = lax.rem(me, seqs) * 16 + me // seqs
    snew = jnp.where(lane1 == spot, s1, jnp.where(lane1 == spot + 8, s2, NEG))
    own_head = lax.rem(lane, 8) == sub
    col = lax.broadcasted_iota(jnp.int32, (8, width), 1)
    own_head_wide = lax.rem(col, 8) == lax.broadcasted_iota(jnp.int32, (8, width), 0)
    col = col.astype(jnp.float32)
    lane4 = lax.broadcasted_iota(jnp.int32, (1, seqs), 1)
    ends = ((len_ref[...] - me * span) * 8).astype(jnp.float32)

    def score(b):
        qb = q_scr[pl.ds(b, 8, stride=seqs), :] * HEAD_WIDTH**-0.5
        q1 = jnp.where(lane < HEAD_WIDTH, qb, 0.0)
        q2 = jnp.where(lane >= HEAD_WIDTH, qb, 0.0)
        q16 = jnp.concatenate([q1, q2], axis=0).astype(jnp.bfloat16)
        return lax.dot_general(
            q16, key_ref[b], (((1,), (1,)), ((), ())), preferred_element_type=jnp.float32
        )

    def weigh(b, s):
        limit = jnp.sum(jnp.where(lane4 == b, ends, 0.0), axis=1, keepdims=True)
        live = jnp.logical_and(own_head_wide, col < limit)
        weights = []
        for m in range(2):
            part = jnp.where(live, s[m * 8 : (m + 1) * 8], NEG)
            hi, lo = two_pieces(jnp.max(part, axis=1, keepdims=True))
            w = jnp.where(live, jnp.exp(part - (hi + lo)), 0.0)
            lhi, llo = two_pieces(jnp.sum(w, axis=1, keepdims=True))
            weights.append(w)
            r = b * 16 + m * 8
            col_scr[r : r + 8, :] = jnp.where(
                lane == 0, hi, jnp.where(lane == 1, lo, jnp.where(lane == 2, lhi, llo))
            )
        return jnp.concatenate(weights, axis=0).astype(jnp.bfloat16)

    def values(b, w):
        return jnp.dot(w, val_ref[b], preferred_element_type=jnp.float32)

    scores = [score(b) for b in range(seqs)]
    weights = [weigh(b, scores[b]) for b in range(seqs)]
    accs = [values(b, weights[b]) for b in range(seqs)]
    turned = jnp.concatenate([col_scr[...], jnp.zeros_like(col_scr)], axis=0).T
    shi, slo = two_pieces(snew)
    tail = jnp.concatenate(
        [turned[0:4], shi, slo, nk.astype(jnp.float32), nv.astype(jnp.float32)], axis=0
    )
    packed = jnp.concatenate(accs + [tail], axis=0).astype(jnp.bfloat16)
    for j in range(out_ref.shape[0]):
        out_ref[j] = packed


def tails(got_ref):
    peers = got_ref.shape[0]
    tiles = [got_ref[j, ROW_M : ROW_M + 8, :].astype(jnp.float32) for j in range(peers)]
    return lambda r: jnp.concatenate([t[r - ROW_M : r - ROW_M + 1] for t in tiles], axis=0)


def columns(rows):
    used = sum(r.shape[0] for r in rows)
    return jnp.concatenate(rows + [jnp.zeros((128 - used, 128), jnp.float32)], axis=0).T


def weighted(got_ref, scale, r):
    acc = scale[r : r + 8, 0:1] * got_ref[0, r : r + 8, :].astype(jnp.float32)
    for j in range(1, got_ref.shape[0]):
        acc = acc + scale[r : r + 8, j : j + 1] * got_ref[j, r : r + 8, :].astype(jnp.float32)
    return acc


def merge_first(got_ref, out_ref):
    peers = got_ref.shape[0]
    row = tails(got_ref)
    top = row(ROW_M) + row(ROW_M + 1)
    part = row(ROW_L) + row(ROW_L + 1)
    snew = row(ROW_S) + row(ROW_S + 1)
    peak = jnp.max(jnp.maximum(top, snew), axis=0, keepdims=True)
    factor = jnp.exp(top - peak)
    fresh = jnp.sum(jnp.where(snew > 0.5 * NEG, jnp.exp(snew - peak), 0.0), axis=0, keepdims=True)
    total = jnp.sum(part * factor, axis=0, keepdims=True) + fresh
    scale = columns([factor, jnp.broadcast_to(fresh, (8, 128))])
    nk, nv = row(ROW_NK), row(ROW_NV)
    accs = []
    for r in range(0, ROW_M, 8):
        accs.append(weighted(got_ref, scale, r) + scale[r : r + 8, peers : peers + 1] * nv)
    tail = jnp.concatenate(
        [*two_pieces(peak), *two_pieces(total), jnp.zeros((4, 128), jnp.float32)], axis=0
    )
    packed = jnp.concatenate(accs + [tail, nk, nv], axis=0).astype(jnp.bfloat16)
    for j in range(out_ref.shape[0]):
        out_ref[j] = packed


def by_seq(scr, seqs):
    rows = [scr[pl.ds(h, seqs, stride=8), :] for h in range(8)]
    return jnp.concatenate(rows, axis=1).astype(jnp.bfloat16)


def merge_last(got_ref, lam_ref, gain_ref, wo_ref, part_ref, nk_ref, nv_ref, head_scr):
    seqs = nk_ref.shape[0]
    for dst, r in ((nk_ref, ROW_NKS), (nv_ref, ROW_NVS)):
        for b in range(seqs):
            head_scr[b * 8 : b * 8 + 8, :] = got_ref[b, r : r + 8, :].astype(jnp.float32)
        dst[...] = by_seq(head_scr, seqs)
    row = tails(got_ref)
    top = row(ROW_M) + row(ROW_M + 1)
    part = row(ROW_L) + row(ROW_L + 1)
    factor = jnp.exp(top - jnp.max(top, axis=0, keepdims=True))
    total = jnp.sum(part * factor, axis=0, keepdims=True)
    scale = columns([factor / total])
    lane8 = lax.broadcasted_iota(jnp.int32, (8, 8), 1)
    sub8 = lax.broadcasted_iota(jnp.int32, (8, 8), 0)
    lam = jnp.sum(jnp.where(lane8 == sub8, lam_ref[...], 0.0), axis=1, keepdims=True)
    for b in range(seqs):
        mixed = weighted(got_ref, scale, b * 16) - lam * weighted(got_ref, scale, b * 16 + 8)
        mean = jnp.mean(mixed * mixed, axis=1, keepdims=True)
        head_scr[b * 8 : b * 8 + 8, :] = mixed * lax.rsqrt(mean + EPS) * gain_ref[...]
    heads = by_seq(head_scr, seqs)
    part_ref[...] = lax.dot_general(
        heads, wo_ref[...], (((1,), (1,)), ((), ())), preferred_element_type=jnp.float32
    ).astype(jnp.bfloat16)


def finish(part_ref, other_ref, nk_ref, nv_ref, out, nk_out, nv_out, sum_ref, sems):
    copies = [
        pltpu.make_async_copy(src, dst, sems.at[i])
        for i, (src, dst) in enumerate(((nk_ref, nk_out), (nv_ref, nv_out), (sum_ref, out)))
    ]
    copies[0].start()
    copies[1].start()
    total = part_ref[...].astype(jnp.float32) + other_ref[...].astype(jnp.float32)
    sum_ref[...] = total.astype(sum_ref.dtype)
    copies[2].start()
    for c in copies:
        c.wait()


HB = pl.BlockSpec(memory_space=pltpu.HBM)
VM = pl.BlockSpec(memory_space=pltpu.VMEM)


KV = ("kv_0", "kv_1")


def exchange(array, axis):
    return lax.all_to_all(array, axis, split_axis=0, concat_axis=0, tiled=True)


def per_device(
    tokens, norm_gain, w_query, w_key, w_value, w_output, key_cache, value_cache, lengths, lam, head_gain
):
    peers = lax.axis_size(KV)
    seqs, span, heads, width = key_cache.shape
    sent = pl.pallas_call(
        project,
        out_shape=jax.ShapeDtypeStruct((peers, heads + 1, seqs, 128), jnp.int16),
        in_specs=[pl.BlockSpec(memory_space=pltpu.HBM)] * 5,
        out_specs=VM,
        scratch_shapes=[
            pltpu.VMEM(tokens.shape, jnp.bfloat16),
            pltpu.VMEM((1, norm_gain.shape[0]), jnp.float32),
            pltpu.VMEM(w_query.shape, jnp.bfloat16),
            pltpu.VMEM(w_query.shape, jnp.bfloat16),
            pltpu.VMEM(w_query.shape, jnp.bfloat16),
            pltpu.SemaphoreType.DMA((5,)),
        ],
        name="project",
        cost_estimate=pl.CostEstimate(flops=5_000_000_000, bytes_accessed=30_000_000, transcendentals=0),
        compiler_params=pltpu.CompilerParams(vmem_limit_bytes=8 << 20),
    )(*(pltpu.with_memory_space_constraint(a, pltpu.HBM) for a in (tokens, norm_gain.reshape(1, -1), w_query, w_key, w_value)))
    got = exchange(sent, KV)
    sent = pl.pallas_call(
        attend,
        out_shape=jax.ShapeDtypeStruct((lax.axis_size("kv_0"), ROWS_C, 128), jnp.bfloat16),
        in_specs=[VM] * 4,
        out_specs=VM,
        scratch_shapes=[
            pltpu.VMEM((32, 128), jnp.float32),
            pltpu.VMEM((64, 128), jnp.float32),
        ],
        name="attend",
        compiler_params=pltpu.CompilerParams(vmem_limit_bytes=24 << 20),
    )(
        got,
        key_cache.reshape(seqs, span * heads, width),
        value_cache.reshape(seqs, span * heads, width),
        lengths.reshape(1, -1),
    )
    got = exchange(sent, "kv_0")
    sent = pl.pallas_call(
        merge_first,
        out_shape=jax.ShapeDtypeStruct((lax.axis_size("kv_1"), ROWS_E, 128), jnp.bfloat16),
        in_specs=[VM],
        out_specs=VM,
        name="merge_first",
        compiler_params=pltpu.CompilerParams(vmem_limit_bytes=8 << 20),
    )(got)
    got = exchange(sent, "kv_1")
    row = jax.ShapeDtypeStruct((seqs, heads * width), jnp.bfloat16)
    part, new_key, new_value = pl.pallas_call(
        merge_last,
        out_shape=(jax.ShapeDtypeStruct((seqs, w_output.shape[1]), jnp.bfloat16),) + (pltpu.VMEM(row.shape, row.dtype),) * 2,
        in_specs=[VM] * 4,
        out_specs=(VM, VM, VM),
        scratch_shapes=[
            pltpu.VMEM((32, 128), jnp.float32),
        ],
        name="merge_last",
        compiler_params=pltpu.CompilerParams(vmem_limit_bytes=8 << 20),
    )(got, lam.reshape(1, -1), head_gain.reshape(1, -1), w_output.T)
    other = lax.ppermute(part, "tp", [(0, 1), (1, 0)])
    attended, new_key, new_value = pl.pallas_call(
        finish,
        out_shape=(jax.ShapeDtypeStruct(part.shape, part.dtype), row, row),
        in_specs=[VM] * 4,
        out_specs=(HB, HB, HB),
        scratch_shapes=[pltpu.VMEM(part.shape, part.dtype), pltpu.SemaphoreType.DMA((3,))],
        name="finish",
        compiler_params=pltpu.CompilerParams(vmem_limit_bytes=8 << 20),
    )(part, other, new_key, new_value)
    return (attended, new_key, new_value)


def solution(mesh):
    split = Mesh(
        mesh.devices.reshape(mesh.shape["dp"], 8, 4, mesh.shape["tp"]), ("dp", "kv_0", "kv_1", "tp")
    )
    return jax.shard_map(
        per_device,
        mesh=split,
        in_specs=(
            P("dp", KV),
            P(KV),
            P(KV, "tp"),
            P(KV, "tp"),
            P(KV, "tp"),
            P("tp", KV),
            P("dp", KV, "tp", None),
            P("dp", KV, "tp", None),
            P("dp"),
            P("tp"),
            P(),
        ),
        out_specs=(P("dp", KV), P("dp", "tp"), P("dp", "tp")),
        check_vma=False,
    )
```

```python
import jax
import jax.numpy as jnp
from jax import lax
from jax.experimental import pallas as pl
from jax.experimental.pallas import tpu as pltpu
from jax.sharding import Mesh
from jax.sharding import PartitionSpec as P

D = 2048
HEAD_WIDTH = 64
EPS = 1e-6
NEG = -1e30

BITS = 14.5
ROW_M, ROW_L, ROW_S, ROW_NK, ROW_NV, ROWS_C = 64, 66, 68, 70, 71, 72
ROW_NKS, ROW_NVS, ROWS_E = 72, 80, 88

def exponent(a):
    return jnp.ceil(jnp.log2(jnp.maximum(a, 1e-30)))


def project(tok_hbm, gain_hbm, wq_hbm, wk_hbm, wv_hbm, out_ref, tok_ref, gain_ref, wq_ref, wk_ref, wv_ref, sems):
    copies = [
        pltpu.make_async_copy(src, dst, sems.at[i])
        for i, (src, dst) in enumerate(
            [(tok_hbm, tok_ref), (gain_hbm, gain_ref), (wq_hbm, wq_ref), (wk_hbm, wk_ref), (wv_hbm, wv_ref)]
        )
    ]
    for c in copies:
        c.start()
    for c in copies:
        c.wait()
    peers = out_ref.shape[0]
    x = tok_ref[...].astype(jnp.float32)
    seqs = x.shape[0]
    squares = jnp.sum(x * x, axis=-1, keepdims=True)
    scaled = (x * gain_ref[...]).astype(jnp.bfloat16)
    heads = wq_ref.shape[1] // 128

    def rows(w_ref):
        y = jnp.dot(scaled, w_ref[...], preferred_element_type=jnp.float32)
        e = exponent(jnp.max(jnp.abs(y), axis=1, keepdims=True))
        y = jnp.round(y * jnp.exp2(BITS - e))
        return jnp.concatenate([y[:, h * 128 : (h + 1) * 128] for h in range(heads)], axis=0), e

    (q, qe), (k, ke), (v, ve) = rows(wq_ref), rows(wk_ref), rows(wv_ref)
    se = exponent(squares)
    size = squares * jnp.exp2(BITS - se)
    whole = jnp.floor(size)
    rest = jnp.round((size - whole) * 2.0**14)
    lane = lax.broadcasted_iota(jnp.int32, (seqs, 128), 1)
    sub = lax.broadcasted_iota(jnp.int32, (seqs, 128), 0)
    meta = jnp.where(
        lane == 0, qe, jnp.where(lane == 1, se, jnp.where(lane == 2, whole, rest))
    )
    metas = [
        jnp.where(lane == 4, jnp.where(sub < 2, ke[b : b + 1], ve[b : b + 1]), meta)
        for b in range(seqs)
    ]
    q = q.astype(jnp.int32).astype(jnp.int16)
    kr, vr = pltpu.roll(k, 64, 1), pltpu.roll(v, 64, 1)
    for i in range(peers):
        j = i % 8 * seqs + i // 8
        tile = jnp.concatenate([kr[j : j + 1], k[j : j + 1], vr[j : j + 1], v[j : j + 1]], axis=0)
        tile = jnp.where(lane < 64, metas[j % seqs], tile)
        for h in range(heads):
            out_ref[i, h] = q[h * seqs : (h + 1) * seqs]
        out_ref[i, heads] = tile.astype(jnp.int32).astype(jnp.int16)


def two_pieces(a):
    hi = a.astype(jnp.bfloat16).astype(jnp.float32)
    return hi, (a - hi).astype(jnp.bfloat16).astype(jnp.float32)


def attend(got_ref, key_ref, val_ref, len_ref, out_ref, q_scr, col_scr):
    peers = got_ref.shape[0]
    seqs = key_ref.shape[0]
    width = key_ref.shape[1]
    span = width // 8
    me = lax.axis_index("kv_0") * lax.axis_size("kv_1") + lax.axis_index("kv_1")
    total = [jnp.zeros((8, 128), jnp.float32)] * 8
    own = jnp.zeros((8, 128), jnp.float32)
    squares = jnp.zeros((8, 128), jnp.float32)
    for j in range(0, peers, 2):
        got = [
            jnp.concatenate([got_ref[j, i].astype(jnp.int32), got_ref[j + 1, i].astype(jnp.int32)], axis=0)
            for i in range(9)
        ]
        got = [g.astype(jnp.float32) for g in got]
        tile = got[8]
        unit = jnp.exp2(tile - BITS)
        total = [t + g * unit[:, 0:1] for t, g in zip(total, got)]
        own = own + tile * unit[:, 4:5]
        size = tile + pltpu.roll(tile, 127, 1) * 2.0**-14
        squares = squares + size * pltpu.roll(unit, 1, 1)
    total = [t[:seqs] + t[seqs:] for t in total]
    own = own[:seqs] + own[seqs:]
    squares = squares[:seqs] + squares[seqs:]
    lane1 = lax.broadcasted_iota(jnp.int32, (1, 128), 1)
    swap = pltpu.roll(own, 64, 1)
    own_k = jnp.where(lane1 < 64, swap[0:1], own[1:2])
    own_v = jnp.where(lane1 < 64, swap[2:3], own[3:4])
    total = jnp.concatenate(total, axis=0)
    inv = lax.rsqrt(jnp.broadcast_to(squares[:, 2:3], (seqs, 128)) / D + EPS)
    inv8 = jnp.concatenate([inv, inv], axis=0)
    inv32 = jnp.concatenate([inv8] * 4, axis=0)
    q = (total * inv32).astype(jnp.bfloat16).astype(jnp.float32)
    q_scr[...] = q
    seq_id = lax.broadcasted_iota(jnp.int32, (seqs, 128), 0)
    mine = jnp.sum(jnp.where(seq_id == lax.rem(me, seqs), inv, 0.0), axis=0, keepdims=True)
    nk = (own_k * mine).astype(jnp.bfloat16)
    nv = (own_v * mine).astype(jnp.bfloat16)
    lane = lax.broadcasted_iota(jnp.int32, (8, 128), 1)
    sub = lax.broadcasted_iota(jnp.int32, (8, 128), 0)
    lane1 = lax.broadcasted_iota(jnp.int32, (1, 128), 1)
    qk = q_scr[pl.ds(me, 1), :] * nk.astype(jnp.float32) * HEAD_WIDTH**-0.5
    s1 = jnp.sum(jnp.where(lane1 < HEAD_WIDTH, qk, 0.0), axis=1, keepdims=True)
    s2 = jnp.sum(jnp.where(lane1 >= HEAD_WIDTH, qk, 0.0), axis=1, keepdims=True)
    spot = lax.rem(me, seqs) * 16 + me // seqs
    snew = jnp.where(lane1 == spot, s1, jnp.where(lane1 == spot + 8, s2, NEG))
    own_head = lax.rem(lane, 8) == sub
    col = lax.broadcasted_iota(jnp.int32, (8, width), 1)
    own_head_wide = lax.rem(col, 8) == lax.broadcasted_iota(jnp.int32, (8, width), 0)
    col = col.astype(jnp.float32)
    lane4 = lax.broadcasted_iota(jnp.int32, (1, seqs), 1)
    ends = ((len_ref[...] - me * span) * 8).astype(jnp.float32)

    def score(b):
        qb = q_scr[pl.ds(b, 8, stride=seqs), :] * HEAD_WIDTH**-0.5
        q1 = jnp.where(lane < HEAD_WIDTH, qb, 0.0)
        q2 = jnp.where(lane >= HEAD_WIDTH, qb, 0.0)
        q16 = jnp.concatenate([q1, q2], axis=0).astype(jnp.bfloat16)
        return lax.dot_general(
            q16, key_ref[b], (((1,), (1,)), ((), ())), preferred_element_type=jnp.float32
        )

    def weigh(b, s):
        limit = jnp.sum(jnp.where(lane4 == b, ends, 0.0), axis=1, keepdims=True)
        live = jnp.logical_and(own_head_wide, col < limit)
        weights = []
        for m in range(2):
            part = jnp.where(live, s[m * 8 : (m + 1) * 8], NEG)
            hi, lo = two_pieces(jnp.max(part, axis=1, keepdims=True))
            w = jnp.where(live, jnp.exp(part - (hi + lo)), 0.0)
            lhi, llo = two_pieces(jnp.sum(w, axis=1, keepdims=True))
            weights.append(w)
            r = b * 16 + m * 8
            col_scr[r : r + 8, :] = jnp.where(
                lane == 0, hi, jnp.where(lane == 1, lo, jnp.where(lane == 2, lhi, llo))
            )
        return jnp.concatenate(weights, axis=0).astype(jnp.bfloat16)

    def values(b, w):
        return jnp.dot(w, val_ref[b], preferred_element_type=jnp.float32)

    scores = [score(b) for b in range(seqs)]
    weights = [weigh(b, scores[b]) for b in range(seqs)]
    accs = [values(b, weights[b]) for b in range(seqs)]
    turned = jnp.concatenate([col_scr[...], jnp.zeros_like(col_scr)], axis=0).T
    shi, slo = two_pieces(snew)
    tail = jnp.concatenate(
        [turned[0:4], shi, slo, nk.astype(jnp.float32), nv.astype(jnp.float32)], axis=0
    )
    packed = jnp.concatenate(accs + [tail], axis=0).astype(jnp.bfloat16)
    for j in range(out_ref.shape[0]):
        out_ref[j] = packed


def tails(got_ref):
    peers = got_ref.shape[0]
    tiles = [got_ref[j, ROW_M : ROW_M + 8, :].astype(jnp.float32) for j in range(peers)]
    return lambda r: jnp.concatenate([t[r - ROW_M : r - ROW_M + 1] for t in tiles], axis=0)


def columns(rows):
    used = sum(r.shape[0] for r in rows)
    return jnp.concatenate(rows + [jnp.zeros((128 - used, 128), jnp.float32)], axis=0).T


def weighted(got_ref, scale, r):
    acc = scale[r : r + 8, 0:1] * got_ref[0, r : r + 8, :].astype(jnp.float32)
    for j in range(1, got_ref.shape[0]):
        acc = acc + scale[r : r + 8, j : j + 1] * got_ref[j, r : r + 8, :].astype(jnp.float32)
    return acc


def merge_first(got_ref, out_ref):
    peers = got_ref.shape[0]
    row = tails(got_ref)
    top = row(ROW_M) + row(ROW_M + 1)
    part = row(ROW_L) + row(ROW_L + 1)
    snew = row(ROW_S) + row(ROW_S + 1)
    peak = jnp.max(jnp.maximum(top, snew), axis=0, keepdims=True)
    factor = jnp.exp(top - peak)
    fresh = jnp.sum(jnp.where(snew > 0.5 * NEG, jnp.exp(snew - peak), 0.0), axis=0, keepdims=True)
    total = jnp.sum(part * factor, axis=0, keepdims=True) + fresh
    scale = columns([factor, jnp.broadcast_to(fresh, (8, 128))])
    nk, nv = row(ROW_NK), row(ROW_NV)
    accs = []
    for r in range(0, ROW_M, 8):
        accs.append(weighted(got_ref, scale, r) + scale[r : r + 8, peers : peers + 1] * nv)
    tail = jnp.concatenate(
        [*two_pieces(peak), *two_pieces(total), jnp.zeros((4, 128), jnp.float32)], axis=0
    )
    packed = jnp.concatenate(accs + [tail, nk, nv], axis=0).astype(jnp.bfloat16)
    for j in range(out_ref.shape[0]):
        out_ref[j] = packed


def by_seq(scr, seqs):
    rows = [scr[pl.ds(h, seqs, stride=8), :] for h in range(8)]
    return jnp.concatenate(rows, axis=1).astype(jnp.bfloat16)


def merge_last(got_ref, lam_ref, gain_ref, wo_ref, part_ref, nk_ref, nv_ref, head_scr):
    seqs = nk_ref.shape[0]
    for dst, r in ((nk_ref, ROW_NKS), (nv_ref, ROW_NVS)):
        for b in range(seqs):
            head_scr[b * 8 : b * 8 + 8, :] = got_ref[b, r : r + 8, :].astype(jnp.float32)
        dst[...] = by_seq(head_scr, seqs)
    row = tails(got_ref)
    top = row(ROW_M) + row(ROW_M + 1)
    part = row(ROW_L) + row(ROW_L + 1)
    factor = jnp.exp(top - jnp.max(top, axis=0, keepdims=True))
    total = jnp.sum(part * factor, axis=0, keepdims=True)
    scale = columns([factor / total])
    lane8 = lax.broadcasted_iota(jnp.int32, (8, 8), 1)
    sub8 = lax.broadcasted_iota(jnp.int32, (8, 8), 0)
    lam = jnp.sum(jnp.where(lane8 == sub8, lam_ref[...], 0.0), axis=1, keepdims=True)
    for b in range(seqs):
        mixed = weighted(got_ref, scale, b * 16) - lam * weighted(got_ref, scale, b * 16 + 8)
        mean = jnp.mean(mixed * mixed, axis=1, keepdims=True)
        head_scr[b * 8 : b * 8 + 8, :] = mixed * lax.rsqrt(mean + EPS) * gain_ref[...]
    heads = by_seq(head_scr, seqs)
    part_ref[...] = lax.dot_general(
        heads, wo_ref[...], (((1,), (1,)), ((), ())), preferred_element_type=jnp.float32
    ).astype(jnp.bfloat16)


def finish(part_ref, other_ref, nk_ref, nv_ref, out, nk_out, nv_out, sum_ref, sems):
    copies = [
        pltpu.make_async_copy(src, dst, sems.at[i])
        for i, (src, dst) in enumerate(((nk_ref, nk_out), (nv_ref, nv_out), (sum_ref, out)))
    ]
    copies[0].start()
    copies[1].start()
    total = part_ref[...].astype(jnp.float32) + other_ref[...].astype(jnp.float32)
    sum_ref[...] = total.astype(sum_ref.dtype)
    copies[2].start()
    for c in copies:
        c.wait()


HB = pl.BlockSpec(memory_space=pltpu.HBM)
VM = pl.BlockSpec(memory_space=pltpu.VMEM)


KV = ("kv_0", "kv_1")


def exchange(array, axis):
    return lax.all_to_all(array, axis, split_axis=0, concat_axis=0, tiled=True)


def per_device(
    tokens, norm_gain, w_query, w_key, w_value, w_output, key_cache, value_cache, lengths, lam, head_gain
):
    peers = lax.axis_size(KV)
    seqs, span, heads, width = key_cache.shape
    sent = pl.pallas_call(
        project,
        out_shape=jax.ShapeDtypeStruct((peers, heads + 1, seqs, 128), jnp.int16),
        in_specs=[pl.BlockSpec(memory_space=pltpu.HBM)] * 5,
        out_specs=VM,
        scratch_shapes=[
            pltpu.VMEM(tokens.shape, jnp.bfloat16),
            pltpu.VMEM((1, norm_gain.shape[0]), jnp.float32),
            pltpu.VMEM(w_query.shape, jnp.bfloat16),
            pltpu.VMEM(w_query.shape, jnp.bfloat16),
            pltpu.VMEM(w_query.shape, jnp.bfloat16),
            pltpu.SemaphoreType.DMA((5,)),
        ],
        name="project",
        compiler_params=pltpu.CompilerParams(vmem_limit_bytes=8 << 20),
    )(*(pltpu.with_memory_space_constraint(a, pltpu.HBM) for a in (tokens, norm_gain.reshape(1, -1), w_query, w_key, w_value)))
    sent = pl.pallas_call(
        lambda given, same: None,
        out_shape=jax.ShapeDtypeStruct(sent.shape, sent.dtype),
        in_specs=[pl.BlockSpec(memory_space=pl.ANY)],
        out_specs=pl.BlockSpec(memory_space=pl.ANY),
        input_output_aliases={0: 0},
        name="hold",
        cost_estimate=pl.CostEstimate(flops=5_000_000_000, bytes_accessed=30_000_000, transcendentals=0),
        compiler_params=pltpu.CompilerParams(vmem_limit_bytes=1 << 20),
    )(sent)
    got = exchange(sent, KV[::-1])
    sent = pl.pallas_call(
        attend,
        out_shape=jax.ShapeDtypeStruct((lax.axis_size("kv_0"), ROWS_C, 128), jnp.bfloat16),
        in_specs=[VM] * 4,
        out_specs=VM,
        scratch_shapes=[
            pltpu.VMEM((32, 128), jnp.float32),
            pltpu.VMEM((64, 128), jnp.float32),
        ],
        name="attend",
        compiler_params=pltpu.CompilerParams(vmem_limit_bytes=24 << 20),
    )(
        got,
        key_cache.reshape(seqs, span * heads, width),
        value_cache.reshape(seqs, span * heads, width),
        lengths.reshape(1, -1),
    )
    got = exchange(sent, "kv_0")
    sent = pl.pallas_call(
        merge_first,
        out_shape=jax.ShapeDtypeStruct((lax.axis_size("kv_1"), ROWS_E, 128), jnp.bfloat16),
        in_specs=[VM],
        out_specs=VM,
        name="merge_first",
        compiler_params=pltpu.CompilerParams(vmem_limit_bytes=8 << 20),
    )(got)
    got = exchange(sent, "kv_1")
    row = jax.ShapeDtypeStruct((seqs, heads * width), jnp.bfloat16)
    part, new_key, new_value = pl.pallas_call(
        merge_last,
        out_shape=(jax.ShapeDtypeStruct((seqs, w_output.shape[1]), jnp.bfloat16),) + (pltpu.VMEM(row.shape, row.dtype),) * 2,
        in_specs=[VM] * 4,
        out_specs=(VM, VM, VM),
        scratch_shapes=[
            pltpu.VMEM((32, 128), jnp.float32),
        ],
        name="merge_last",
        compiler_params=pltpu.CompilerParams(vmem_limit_bytes=8 << 20),
    )(got, lam.reshape(1, -1), head_gain.reshape(1, -1), w_output.T)
    other = lax.ppermute(part, "tp", [(0, 1), (1, 0)])
    attended, new_key, new_value = pl.pallas_call(
        finish,
        out_shape=(jax.ShapeDtypeStruct(part.shape, part.dtype), row, row),
        in_specs=[VM] * 4,
        out_specs=(HB, HB, HB),
        scratch_shapes=[pltpu.VMEM(part.shape, part.dtype), pltpu.SemaphoreType.DMA((3,))],
        name="finish",
        compiler_params=pltpu.CompilerParams(vmem_limit_bytes=8 << 20),
    )(part, other, new_key, new_value)
    return (attended, new_key, new_value)


def solution(mesh):
    split = Mesh(
        mesh.devices.reshape(mesh.shape["dp"], 8, 4, mesh.shape["tp"]), ("dp", "kv_0", "kv_1", "tp")
    )
    return jax.shard_map(
        per_device,
        mesh=split,
        in_specs=(
            P("dp", KV),
            P(KV),
            P(KV, "tp"),
            P(KV, "tp"),
            P(KV, "tp"),
            P("tp", KV),
            P("dp", KV, "tp", None),
            P("dp", KV, "tp", None),
            P("dp"),
            P("tp"),
            P(),
        ),
        out_specs=(P("dp", KV), P("dp", "tp"), P("dp", "tp")),
        check_vma=False,
    )
```

```python
import jax
import jax.numpy as jnp
from jax import lax
from jax.experimental import pallas as pl
from jax.experimental.pallas import tpu as pltpu
from jax.sharding import Mesh
from jax.sharding import PartitionSpec as P

D = 2048
HEAD_WIDTH = 64
EPS = 1e-6
NEG = -1e30

BITS = 14.5
ROW_M, ROW_L, ROW_S, ROW_NK, ROW_NV, ROWS_C = 64, 66, 68, 70, 71, 72
ROW_NKS, ROW_NVS, ROWS_E = 72, 80, 88

def exponent(a):
    return jnp.ceil(jnp.log2(jnp.maximum(a, 1e-30)))


def project(tok_hbm, gain_hbm, wq_hbm, wk_hbm, wv_hbm, out_ref, tok_ref, gain_ref, wq_ref, wk_ref, wv_ref, sems):
    copies = [
        pltpu.make_async_copy(src, dst, sems.at[i])
        for i, (src, dst) in enumerate(
            [(tok_hbm, tok_ref), (gain_hbm, gain_ref), (wq_hbm, wq_ref), (wk_hbm, wk_ref), (wv_hbm, wv_ref)]
        )
    ]
    for c in copies:
        c.start()
    for c in copies:
        c.wait()
    peers = out_ref.shape[0]
    x = tok_ref[...].astype(jnp.float32)
    seqs = x.shape[0]
    squares = jnp.sum(x * x, axis=-1, keepdims=True)
    scaled = (x * gain_ref[...]).astype(jnp.bfloat16)
    heads = wq_ref.shape[1] // 128

    def rows(w_ref):
        y = jnp.dot(scaled, w_ref[...], preferred_element_type=jnp.float32)
        e = exponent(jnp.max(jnp.abs(y), axis=1, keepdims=True))
        y = jnp.round(y * jnp.exp2(BITS - e))
        return jnp.concatenate([y[:, h * 128 : (h + 1) * 128] for h in range(heads)], axis=0), e

    (q, qe), (k, ke), (v, ve) = rows(wq_ref), rows(wk_ref), rows(wv_ref)
    se = exponent(squares)
    size = squares * jnp.exp2(BITS - se)
    whole = jnp.floor(size)
    rest = jnp.round((size - whole) * 2.0**14)
    lane = lax.broadcasted_iota(jnp.int32, (seqs, 128), 1)
    sub = lax.broadcasted_iota(jnp.int32, (seqs, 128), 0)
    meta = jnp.where(
        lane == 0, qe, jnp.where(lane == 1, se, jnp.where(lane == 2, whole, rest))
    )
    metas = [
        jnp.where(lane == 4, jnp.where(sub < 2, ke[b : b + 1], ve[b : b + 1]), meta)
        for b in range(seqs)
    ]
    q = q.astype(jnp.int32).astype(jnp.int16)
    kr, vr = pltpu.roll(k, 64, 1), pltpu.roll(v, 64, 1)
    for i in range(peers):
        j = i % 8 * seqs + i // 8
        tile = jnp.concatenate([kr[j : j + 1], k[j : j + 1], vr[j : j + 1], v[j : j + 1]], axis=0)
        tile = jnp.where(lane < 64, metas[j % seqs], tile)
        for h in range(heads):
            out_ref[i, h] = q[h * seqs : (h + 1) * seqs]
        out_ref[i, heads] = tile.astype(jnp.int32).astype(jnp.int16)


def two_pieces(a):
    hi = a.astype(jnp.bfloat16).astype(jnp.float32)
    return hi, (a - hi).astype(jnp.bfloat16).astype(jnp.float32)


def attend(got_ref, key_ref, val_ref, len_ref, out_ref, q_scr, col_scr):
    peers = got_ref.shape[0]
    seqs = key_ref.shape[0]
    width = key_ref.shape[1]
    span = width // 8
    me = lax.axis_index("kv_0") * lax.axis_size("kv_1") + lax.axis_index("kv_1")
    total = [jnp.zeros((8, 128), jnp.float32)] * 8
    own = jnp.zeros((8, 128), jnp.float32)
    squares = jnp.zeros((8, 128), jnp.float32)
    for j in range(0, peers, 2):
        got = [
            jnp.concatenate([got_ref[j, i].astype(jnp.int32), got_ref[j + 1, i].astype(jnp.int32)], axis=0)
            for i in range(9)
        ]
        got = [g.astype(jnp.float32) for g in got]
        tile = got[8]
        unit = jnp.exp2(tile - BITS)
        total = [t + g * unit[:, 0:1] for t, g in zip(total, got)]
        own = own + tile * unit[:, 4:5]
        size = tile + pltpu.roll(tile, 127, 1) * 2.0**-14
        squares = squares + size * pltpu.roll(unit, 1, 1)
    total = [t[:seqs] + t[seqs:] for t in total]
    own = own[:seqs] + own[seqs:]
    squares = squares[:seqs] + squares[seqs:]
    lane1 = lax.broadcasted_iota(jnp.int32, (1, 128), 1)
    swap = pltpu.roll(own, 64, 1)
    own_k = jnp.where(lane1 < 64, swap[0:1], own[1:2])
    own_v = jnp.where(lane1 < 64, swap[2:3], own[3:4])
    total = jnp.concatenate(total, axis=0)
    inv = lax.rsqrt(jnp.broadcast_to(squares[:, 2:3], (seqs, 128)) / D + EPS)
    inv8 = jnp.concatenate([inv, inv], axis=0)
    inv32 = jnp.concatenate([inv8] * 4, axis=0)
    q = (total * inv32).astype(jnp.bfloat16).astype(jnp.float32)
    q_scr[...] = q
    seq_id = lax.broadcasted_iota(jnp.int32, (seqs, 128), 0)
    mine = jnp.sum(jnp.where(seq_id == lax.rem(me, seqs), inv, 0.0), axis=0, keepdims=True)
    nk = (own_k * mine).astype(jnp.bfloat16)
    nv = (own_v * mine).astype(jnp.bfloat16)
    lane = lax.broadcasted_iota(jnp.int32, (8, 128), 1)
    sub = lax.broadcasted_iota(jnp.int32, (8, 128), 0)
    lane1 = lax.broadcasted_iota(jnp.int32, (1, 128), 1)
    qk = q_scr[pl.ds(me, 1), :] * nk.astype(jnp.float32) * HEAD_WIDTH**-0.5
    s1 = jnp.sum(jnp.where(lane1 < HEAD_WIDTH, qk, 0.0), axis=1, keepdims=True)
    s2 = jnp.sum(jnp.where(lane1 >= HEAD_WIDTH, qk, 0.0), axis=1, keepdims=True)
    spot = lax.rem(me, seqs) * 16 + me // seqs
    snew = jnp.where(lane1 == spot, s1, jnp.where(lane1 == spot + 8, s2, NEG))
    own_head = lax.rem(lane, 8) == sub
    col = lax.broadcasted_iota(jnp.int32, (8, width), 1)
    own_head_wide = lax.rem(col, 8) == lax.broadcasted_iota(jnp.int32, (8, width), 0)
    col = col.astype(jnp.float32)
    lane4 = lax.broadcasted_iota(jnp.int32, (1, seqs), 1)
    ends = ((len_ref[...] - me * span) * 8).astype(jnp.float32)

    def score(b):
        qb = q_scr[pl.ds(b, 8, stride=seqs), :] * HEAD_WIDTH**-0.5
        q1 = jnp.where(lane < HEAD_WIDTH, qb, 0.0)
        q2 = jnp.where(lane >= HEAD_WIDTH, qb, 0.0)
        q16 = jnp.concatenate([q1, q2], axis=0).astype(jnp.bfloat16)
        return lax.dot_general(
            q16, key_ref[b], (((1,), (1,)), ((), ())), preferred_element_type=jnp.float32
        )

    def weigh(b, s):
        limit = jnp.sum(jnp.where(lane4 == b, ends, 0.0), axis=1, keepdims=True)
        live = jnp.logical_and(own_head_wide, col < limit)
        weights = []
        for m in range(2):
            part = jnp.where(live, s[m * 8 : (m + 1) * 8], NEG)
            hi, lo = two_pieces(jnp.max(part, axis=1, keepdims=True))
            w = jnp.where(live, jnp.exp(part - (hi + lo)), 0.0)
            lhi, llo = two_pieces(jnp.sum(w, axis=1, keepdims=True))
            weights.append(w)
            r = b * 16 + m * 8
            col_scr[r : r + 8, :] = jnp.where(
                lane == 0, hi, jnp.where(lane == 1, lo, jnp.where(lane == 2, lhi, llo))
            )
        return jnp.concatenate(weights, axis=0).astype(jnp.bfloat16)

    def values(b, w):
        return jnp.dot(w, val_ref[b], preferred_element_type=jnp.float32)

    scores = [score(b) for b in range(seqs)]
    weights = [weigh(b, scores[b]) for b in range(seqs)]
    accs = [values(b, weights[b]) for b in range(seqs)]
    turned = jnp.concatenate([col_scr[...], jnp.zeros_like(col_scr)], axis=0).T
    shi, slo = two_pieces(snew)
    tail = jnp.concatenate(
        [turned[0:4], shi, slo, nk.astype(jnp.float32), nv.astype(jnp.float32)], axis=0
    )
    packed = jnp.concatenate(accs + [tail], axis=0).astype(jnp.bfloat16)
    for j in range(out_ref.shape[0]):
        out_ref[j] = packed


def tails(got_ref):
    peers = got_ref.shape[0]
    tiles = [got_ref[j, ROW_M : ROW_M + 8, :].astype(jnp.float32) for j in range(peers)]
    return lambda r: jnp.concatenate([t[r - ROW_M : r - ROW_M + 1] for t in tiles], axis=0)


def columns(rows):
    used = sum(r.shape[0] for r in rows)
    return jnp.concatenate(rows + [jnp.zeros((128 - used, 128), jnp.float32)], axis=0).T


def weighted(got_ref, scale, r):
    acc = scale[r : r + 8, 0:1] * got_ref[0, r : r + 8, :].astype(jnp.float32)
    for j in range(1, got_ref.shape[0]):
        acc = acc + scale[r : r + 8, j : j + 1] * got_ref[j, r : r + 8, :].astype(jnp.float32)
    return acc


def merge_first(got_ref, out_ref):
    peers = got_ref.shape[0]
    row = tails(got_ref)
    top = row(ROW_M) + row(ROW_M + 1)
    part = row(ROW_L) + row(ROW_L + 1)
    snew = row(ROW_S) + row(ROW_S + 1)
    peak = jnp.max(jnp.maximum(top, snew), axis=0, keepdims=True)
    factor = jnp.exp(top - peak)
    fresh = jnp.sum(jnp.where(snew > 0.5 * NEG, jnp.exp(snew - peak), 0.0), axis=0, keepdims=True)
    total = jnp.sum(part * factor, axis=0, keepdims=True) + fresh
    scale = columns([factor, jnp.broadcast_to(fresh, (8, 128))])
    nk, nv = row(ROW_NK), row(ROW_NV)
    accs = []
    for r in range(0, ROW_M, 8):
        accs.append(weighted(got_ref, scale, r) + scale[r : r + 8, peers : peers + 1] * nv)
    tail = jnp.concatenate(
        [*two_pieces(peak), *two_pieces(total), jnp.zeros((4, 128), jnp.float32)], axis=0
    )
    packed = jnp.concatenate(accs + [tail, nk, nv], axis=0).astype(jnp.bfloat16)
    for j in range(out_ref.shape[0]):
        out_ref[j] = packed


def by_seq(scr, seqs):
    rows = [scr[pl.ds(h, seqs, stride=8), :] for h in range(8)]
    return jnp.concatenate(rows, axis=1).astype(jnp.bfloat16)


def merge_last(got_ref, lam_ref, gain_ref, wo_ref, part_ref, head_scr):
    seqs = part_ref.shape[0]
    row = tails(got_ref)
    top = row(ROW_M) + row(ROW_M + 1)
    part = row(ROW_L) + row(ROW_L + 1)
    factor = jnp.exp(top - jnp.max(top, axis=0, keepdims=True))
    total = jnp.sum(part * factor, axis=0, keepdims=True)
    scale = columns([factor / total])
    lane8 = lax.broadcasted_iota(jnp.int32, (8, 8), 1)
    sub8 = lax.broadcasted_iota(jnp.int32, (8, 8), 0)
    lam = jnp.sum(jnp.where(lane8 == sub8, lam_ref[...], 0.0), axis=1, keepdims=True)
    for b in range(seqs):
        mixed = weighted(got_ref, scale, b * 16) - lam * weighted(got_ref, scale, b * 16 + 8)
        mean = jnp.mean(mixed * mixed, axis=1, keepdims=True)
        head_scr[b * 8 : b * 8 + 8, :] = mixed * lax.rsqrt(mean + EPS) * gain_ref[...]
    heads = by_seq(head_scr, seqs)
    part_ref[...] = lax.dot_general(
        heads, wo_ref[...], (((1,), (1,)), ((), ())), preferred_element_type=jnp.float32
    ).astype(jnp.bfloat16)


def emit(got_ref, nk_out, nv_out, nk_ref, nv_ref, scr, sems):
    seqs = nk_ref.shape[0]
    copies = []
    for i, (out, dst, r) in enumerate(((nk_out, nk_ref, ROW_NKS), (nv_out, nv_ref, ROW_NVS))):
        for b in range(seqs):
            scr[b * 8 : b * 8 + 8, :] = got_ref[b, r : r + 8, :].astype(jnp.float32)
        dst[...] = by_seq(scr, seqs)
        copies.append(pltpu.make_async_copy(dst, out, sems.at[i]))
        copies[i].start()
    for c in copies:
        c.wait()


def finish(part_ref, other_ref, out_ref):
    total = part_ref[...].astype(jnp.float32) + other_ref[...].astype(jnp.float32)
    out_ref[...] = total.astype(out_ref.dtype)


HB = pl.BlockSpec(memory_space=pltpu.HBM)
VM = pl.BlockSpec(memory_space=pltpu.VMEM)


KV = ("kv_0", "kv_1")


def exchange(array, axis):
    return lax.all_to_all(array, axis, split_axis=0, concat_axis=0, tiled=True)


def per_device(
    tokens, norm_gain, w_query, w_key, w_value, w_output, key_cache, value_cache, lengths, lam, head_gain
):
    peers = lax.axis_size(KV)
    seqs, span, heads, width = key_cache.shape
    sent = pl.pallas_call(
        project,
        out_shape=jax.ShapeDtypeStruct((peers, heads + 1, seqs, 128), jnp.int16),
        in_specs=[pl.BlockSpec(memory_space=pltpu.HBM)] * 5,
        out_specs=VM,
        scratch_shapes=[
            pltpu.VMEM(tokens.shape, jnp.bfloat16),
            pltpu.VMEM((1, norm_gain.shape[0]), jnp.float32),
            pltpu.VMEM(w_query.shape, jnp.bfloat16),
            pltpu.VMEM(w_query.shape, jnp.bfloat16),
            pltpu.VMEM(w_query.shape, jnp.bfloat16),
            pltpu.SemaphoreType.DMA((5,)),
        ],
        name="project",
        compiler_params=pltpu.CompilerParams(vmem_limit_bytes=8 << 20),
    )(*(pltpu.with_memory_space_constraint(a, pltpu.HBM) for a in (tokens, norm_gain.reshape(1, -1), w_query, w_key, w_value)))
    sent = pl.pallas_call(
        lambda given, same: None,
        out_shape=jax.ShapeDtypeStruct(sent.shape, sent.dtype),
        in_specs=[pl.BlockSpec(memory_space=pl.ANY)],
        out_specs=pl.BlockSpec(memory_space=pl.ANY),
        input_output_aliases={0: 0},
        name="hold",
        cost_estimate=pl.CostEstimate(flops=5_000_000_000, bytes_accessed=30_000_000, transcendentals=0),
        compiler_params=pltpu.CompilerParams(vmem_limit_bytes=1 << 20),
    )(sent)
    got = exchange(sent, KV[::-1])
    sent = pl.pallas_call(
        attend,
        out_shape=jax.ShapeDtypeStruct((lax.axis_size("kv_0"), ROWS_C, 128), jnp.bfloat16),
        in_specs=[VM] * 4,
        out_specs=VM,
        scratch_shapes=[
            pltpu.VMEM((32, 128), jnp.float32),
            pltpu.VMEM((64, 128), jnp.float32),
        ],
        name="attend",
        compiler_params=pltpu.CompilerParams(vmem_limit_bytes=24 << 20),
    )(
        got,
        key_cache.reshape(seqs, span * heads, width),
        value_cache.reshape(seqs, span * heads, width),
        lengths.reshape(1, -1),
    )
    got = exchange(sent, "kv_0")
    sent = pl.pallas_call(
        merge_first,
        out_shape=jax.ShapeDtypeStruct((lax.axis_size("kv_1"), ROWS_E, 128), jnp.bfloat16),
        in_specs=[VM],
        out_specs=VM,
        name="merge_first",
        compiler_params=pltpu.CompilerParams(vmem_limit_bytes=8 << 20),
    )(got)
    got = exchange(sent, "kv_1")
    row = jax.ShapeDtypeStruct((seqs, heads * width), jnp.bfloat16)
    part = pl.pallas_call(
        merge_last,
        out_shape=jax.ShapeDtypeStruct((seqs, w_output.shape[1]), jnp.bfloat16),
        in_specs=[VM] * 4,
        out_specs=VM,
        scratch_shapes=[pltpu.VMEM((32, 128), jnp.float32)],
        name="merge_last",
        compiler_params=pltpu.CompilerParams(vmem_limit_bytes=8 << 20),
    )(got, lam.reshape(1, -1), head_gain.reshape(1, -1), w_output.T)
    other = lax.ppermute(part, "tp", [(0, 1), (1, 0)])
    new_key, new_value = pl.pallas_call(
        emit,
        out_shape=(row, row),
        in_specs=[VM],
        out_specs=(HB, HB),
        scratch_shapes=[
            pltpu.VMEM(row.shape, row.dtype),
            pltpu.VMEM(row.shape, row.dtype),
            pltpu.VMEM((32, 128), jnp.float32),
            pltpu.SemaphoreType.DMA((2,)),
        ],
        name="emit",
        cost_estimate=pl.CostEstimate(flops=1_000_000, bytes_accessed=1_000_000, transcendentals=0),
        compiler_params=pltpu.CompilerParams(vmem_limit_bytes=8 << 20),
    )(got)
    attended = pl.pallas_call(
        finish,
        out_shape=jax.ShapeDtypeStruct(part.shape, part.dtype),
        in_specs=[VM] * 2,
        out_specs=VM,
        name="finish",
        compiler_params=pltpu.CompilerParams(vmem_limit_bytes=8 << 20),
    )(part, other)
    return (attended, new_key, new_value)


def solution(mesh):
    split = Mesh(
        mesh.devices.reshape(mesh.shape["dp"], 8, 4, mesh.shape["tp"]), ("dp", "kv_0", "kv_1", "tp")
    )
    return jax.shard_map(
        per_device,
        mesh=split,
        in_specs=(
            P("dp", KV),
            P(KV),
            P(KV, "tp"),
            P(KV, "tp"),
            P(KV, "tp"),
            P("tp", KV),
            P("dp", KV, "tp", None),
            P("dp", KV, "tp", None),
            P("dp"),
            P("tp"),
            P(),
        ),
        out_specs=(P("dp", KV), P("dp", "tp"), P("dp", "tp")),
        check_vma=False,
    )
```
